512 devices in a mesh: sp: 64 (over z, y), fs: 4 (over x), tp: 2 (over core).
Axes of the slice: x: 4, y: 8, z: 8, core: 2. Of those that a mesh axis runs over, the one named last changes fastest.
Arguments:
- tokens: bfloat16 [32768, 2048], P(('fs', 'sp')), may hold values from -6 to 6
- in_gain: float32 [2048], replicated, may hold values from 0.1 to 1.9
- query_weight: bfloat16 [2048, 512], P(None, ('tp', 'fs')), may hold values from -0.17291713 to 0.17291713
- key_weight: bfloat16 [2048, 512], P(None, ('tp', 'fs')), may hold values from -0.17291713 to 0.17291713
- value_weight: bfloat16 [2048, 512], P(None, ('tp', 'fs')), may hold values from -0.125 to 0.125
- rec_query_weight: bfloat16 [2048, 512], P(None, ('tp', 'fs')), may hold values from -0.125 to 0.125
- rec_forget_weight: bfloat16 [2048, 512], P(None, ('tp', 'fs')), may hold values from -0.125 to 0.125
- rec_input_weight: bfloat16 [2048, 512], P(None, ('tp', 'fs')), may hold values from -0.125 to 0.125
- mix_lambda: float32 [4], P('tp'), may hold values from 0.3 to 0.8
- lower_bound: float32 [4, 128], P('tp'), may hold values from 0.9 to 0.9999695
- forget_scale: float32 [32768], P(('fs', 'sp')), may hold values from 0.35 to 24576
- att_gain: float32 [128], replicated, may hold values from 0.1 to 1.9
- recurrence_gain: float32 [128], replicated, may hold values from 0.1 to 1.9
- att_out_weight: bfloat16 [512, 2048], P('tp'), may hold values from -0.1875 to 0.1875
- rec_out_weight: bfloat16 [512, 2048], P('tp'), may hold values from -0.1875 to 0.1875
Outputs:
- mixed_out: bfloat16 [32768, 2048], P(('fs', 'sp'))
- log_weight_sum: float32 [4, 32768], P('tp', ('fs', 'sp'))
The draws below stay inside these ranges and needn't reach their ends.
All inputs are finite; a program needn't handle non-finite values.
Results may differ from the reference program's by a relative error of at most 0.012.
Values may be sent and summed in bfloat16 or wider, within the bound.
A program may use at most 128 MiB of HBM per device.

```python
import math
import jax
import jax.numpy as jnp
from jax import lax

D = 2048
HEADS = 4
DK = 64
DV = 128
BLK = 64
TOK_DEV = 128
LENGTH_PER_SEQ = 8192
SEQS = 4
TOKEN_COUNT_ALL = 32768
N_TP = 2


def drawn_weight(key, salt):
    spread = (D * 10 // 17) ** (-0.5)
    noise = jnp.clip(jax.random.normal(jax.random.fold_in(key, salt), (D, HEADS * 2 * DK), jnp.float32), -4.5, 4.5) * spread
    return jnp.clip(noise, -6.0 * spread, 6.0 * spread).astype(jnp.bfloat16)


def draw_tokens(key, part):
    base = jax.random.normal(jax.random.fold_in(key, 41), (TOKEN_COUNT_ALL, D), jnp.float32)
    return jnp.clip(base, -6.0, 6.0).astype(jnp.bfloat16)


def draw_query_weight(key, part):
    return drawn_weight(key, 51)


def draw_key_weight(key, part):
    return drawn_weight(key, 53)


def draw_lower_bound(key, part):
    first_key, second_key = jax.random.split(jax.random.fold_in(key, 11))
    slower = jax.random.uniform(first_key, (HEADS, DV), jnp.float32) < 0.5
    mixing = jax.random.uniform(second_key, (HEADS, DV), jnp.float32)
    slower_minimum = 0.25 / LENGTH_PER_SEQ
    slow_gap = jnp.exp(math.log(slower_minimum) + mixing * math.log(3.0))
    fast_gap = jnp.exp(math.log(0.04) + mixing * (math.log(0.1) - math.log(0.04)))
    return (1.0 - jnp.where(slower, slow_gap, fast_gap)).astype(jnp.float32)


def draw_forget_scale(key, part):
    key_collection = jax.random.split(jax.random.fold_in(key, 23), 4)
    device_factor = jnp.exp(math.log(0.5) + jax.random.uniform(key_collection[0], (TOKEN_COUNT_ALL // TOK_DEV,), jnp.float32) * math.log(4.0))
    block_factor = jnp.exp(jax.random.uniform(key_collection[1], (TOKEN_COUNT_ALL // BLK,), jnp.float32) * 0.6 - 0.3)
    initial_scale = jnp.repeat(device_factor, TOK_DEV) * jnp.repeat(block_factor, BLK)
    sudden_rows = jax.random.uniform(key_collection[2], (TOKEN_COUNT_ALL,), jnp.float32) < 2.5 / LENGTH_PER_SEQ
    height_per_level = LENGTH_PER_SEQ * (1.0 + 2.0 * jax.random.uniform(key_collection[3], (TOKEN_COUNT_ALL,), jnp.float32))
    return jnp.where(sudden_rows, height_per_level, initial_scale).astype(jnp.float32)


def shard_levels(rng, shape, cuts, least, largest):
    factor_of = 1.0
    for axis_at, shards_of in cuts:
        heights = jax.random.uniform(jax.random.fold_in(jax.random.fold_in(rng, 6), axis_at), (shards_of,), jnp.float32, least / len(cuts), largest / len(cuts))
        factor_of = factor_of * jnp.repeat(jnp.exp(heights), shape[axis_at] // shards_of).reshape((-1,) + (1,) * (len(shape) - 1 - axis_at))
    return factor_of


def bell_draw(rng, extent, scale, reach, cuts=(), kind=jnp.bfloat16):
    values = jax.random.normal(rng, extent, jnp.float32) * scale
    if len(cuts) > 0:
        values = shard_levels(rng, extent, cuts, -0.22, 0.18) * values
    return jnp.clip(values, min=-reach, max=reach).astype(kind)


def setup_inputs(seed: int = 0) -> dict:
    key_of = jax.random.split(jax.random.key(seed), 16)
    return {
        "tokens": draw_tokens(jax.random.fold_in(key_of[15], 71), 0),
        "in_gain": jnp.clip(1.0 + 0.18 * jax.random.normal(key_of[1], (D,), jnp.float32), 0.1, 1.9),
        "query_weight": draw_query_weight(jax.random.fold_in(key_of[15], 71), 0),
        "key_weight": draw_key_weight(jax.random.fold_in(key_of[15], 71), 0),
        "value_weight": bell_draw(key_of[4], (D, HEADS * DV), D ** -0.5, 0.125, ((1, 8),)),
        "rec_query_weight": bell_draw(key_of[5], (D, HEADS * DV), D ** -0.5, 0.125, ((1, 8),)),
        "rec_forget_weight": bell_draw(key_of[6], (D, HEADS * DV), D ** -0.5, 0.125, ((1, 8),)),
        "rec_input_weight": bell_draw(key_of[7], (D, HEADS * DV), D ** -0.5, 0.125, ((1, 8),)),
        "mix_lambda": jnp.clip(0.3 + 0.5 * jax.random.uniform(key_of[8], (HEADS,), jnp.float32) ** shard_levels(key_of[8], (HEADS,), ((0, 2),), -0.2, 0.2), 0.3, 0.8),
        "lower_bound": draw_lower_bound(jax.random.fold_in(key_of[15], 71), 0),
        "forget_scale": draw_forget_scale(jax.random.fold_in(key_of[15], 71), 0),
        "att_gain": jnp.clip(1.0 + 0.18 * jax.random.normal(key_of[11], (DV,), jnp.float32), 0.1, 1.9),
        "recurrence_gain": jnp.clip(1.0 + 0.18 * jax.random.normal(key_of[12], (DV,), jnp.float32), 0.1, 1.9),
        "att_out_weight": bell_draw(key_of[13], (HEADS * DV, D), (2 * HEADS * DV) ** -0.5, 0.1875, ((0, 2),)),
        "rec_out_weight": bell_draw(key_of[14], (HEADS * DV, D), (2 * HEADS * DV) ** -0.5, 0.1875, ((0, 2),)),
    }


EPS = 1e-06
NEG = -1e+30
QUERY_ROWS = 512

def norm_rows(values, gain):
    return values * lax.rsqrt(lax.optimization_barrier(jnp.mean(values * values, axis=-1, keepdims=True)) + EPS) * gain

def to_sequences(rows):
    return rows.reshape(SEQS, LENGTH_PER_SEQ, rows.shape[-1])

def from_sequences(seq_rows):
    return seq_rows.reshape(TOKEN_COUNT_ALL, seq_rows.shape[-1])

def block_recurrence(queries, key_in, value_in, log_forget):
    head_count, row_count, key_width = queries.shape
    block_count = row_count // BLK

    def to_blocks(array_in):
        return array_in.reshape(head_count, block_count, BLK, array_in.shape[-1]).transpose(1, 0, 2, 3)
    causal = jnp.tril(jnp.ones((BLK, BLK), bool))

    def advance(passed_state, inputs):
        query_block, key_block, value_block, l_blk = inputs
        accumulator_sum = jnp.cumsum(l_blk, axis=1)
        cross_block_output = jnp.einsum('sre,sei->sri', query_block * jnp.exp(accumulator_sum), passed_state, precision=lax.Precision.HIGHEST)
        spread = accumulator_sum[:, :, None, :] - accumulator_sum[:, None, :, :]
        decay = jnp.exp(jnp.where(causal[None, :, :, None], spread, -jnp.inf))
        scores = jnp.einsum('htk,htsk,hsk->hts', query_block, decay, key_block, precision=lax.Precision.HIGHEST)
        result = cross_block_output + jnp.einsum('hts,hsv->htv', scores, value_block, precision=lax.Precision.HIGHEST)
        final_log_sum = accumulator_sum[:, -1:, :]
        updated_state = jnp.exp(final_log_sum[:, 0, :])[:, :, None] * passed_state + jnp.einsum('plf,plt->pft', key_block * jnp.exp(final_log_sum - accumulator_sum), value_block, precision=lax.Precision.HIGHEST)
        return (updated_state, result)
    begin_state = jnp.zeros((head_count, key_width, value_in.shape[-1]), jnp.float32)
    end_state, results = lax.scan(advance, begin_state, (to_blocks(queries), to_blocks(key_in), to_blocks(value_in), to_blocks(log_forget)))
    return (end_state, results.transpose(1, 0, 2, 3).reshape(head_count, row_count, value_in.shape[-1]))

def attend_sequence(q_seq, k_seq, v_seq, mix_lambda, att_gain):
    length_now = q_seq.shape[0]
    queries = q_seq.reshape(length_now, HEADS, 2, DK).transpose(1, 2, 0, 3).astype(jnp.float32)
    key_heads = k_seq.reshape(length_now, HEADS, 2, DK).transpose(1, 2, 0, 3).astype(jnp.float32)
    head_values = v_seq.reshape(length_now, HEADS, DV).transpose(1, 0, 2).astype(jnp.float32)
    block_rows = min(QUERY_ROWS, length_now)
    key_pos = jnp.arange(length_now, dtype=jnp.int32)

    def one_block(block_index):
        begin_row = (block_index * block_rows).astype(jnp.int32)
        query_block = lax.dynamic_slice_in_dim(queries, begin_row, block_rows, 2)
        q_pos = begin_row + jnp.arange(block_rows, dtype=jnp.int32)
        allowed = q_pos[:, None] >= key_pos[None, :]
        scores = jnp.einsum('hmqd,hmkd->hmqk', query_block, key_heads) * DK ** (-0.5)
        scores = jnp.where(allowed, scores, NEG)
        highest = lax.optimization_barrier(jnp.max(scores, axis=-1))
        weights = jnp.exp(scores - highest[..., None])
        weight_sum = lax.optimization_barrier(jnp.sum(weights, axis=-1))
        rounded_weights = lax.optimization_barrier(weights.astype(jnp.bfloat16)).astype(jnp.float32)
        summed_values = jnp.einsum('itap,ipn->itan', rounded_weights, head_values)
        mixed = summed_values[:, 0] / weight_sum[:, 0, :, None] - mix_lambda[:, None, None] * summed_values[:, 1] / weight_sum[:, 1, :, None]
        result = (norm_rows(mixed, att_gain) * 0.8).astype(jnp.bfloat16)
        return (result.transpose(1, 0, 2).reshape(block_rows, HEADS * DV), highest[:, 0] + jnp.log(weight_sum[:, 0]))
    results, log_sums = lax.map(one_block, jnp.arange(length_now // block_rows, dtype=jnp.int32))
    return (results.reshape(length_now, HEADS * DV), log_sums.transpose(1, 0, 2).reshape(HEADS, length_now))

def recur_sequence(rq_seq, rf_seq, ri_seq, scale_seq, lower_bound, recurrence_gain):
    length_now = rq_seq.shape[0]

    def heads_first(array_in):
        return array_in.reshape(length_now, HEADS, DV).transpose(1, 0, 2).astype(jnp.float32)
    queries = heads_first(rq_seq)
    lower_edge = lower_bound[:, None, :]
    forget = lower_edge + (1.0 - lower_edge) * jax.nn.sigmoid(heads_first(rf_seq))
    log_forget = scale_seq[None, :, None] * jnp.log(forget)
    key_in = 1.0 - jnp.exp(log_forget)
    _, results = block_recurrence(queries, key_in, heads_first(ri_seq), log_forget)
    normed_out = norm_rows(results, recurrence_gain).astype(jnp.bfloat16)
    return normed_out.transpose(1, 0, 2).reshape(length_now, HEADS * DV)

def reference(tokens, in_gain, query_weight, key_weight, value_weight, rec_query_weight, rec_forget_weight, rec_input_weight, mix_lambda, lower_bound, forget_scale, att_gain, recurrence_gain, att_out_weight, rec_out_weight):
    normed = norm_rows(tokens.astype(jnp.float32), in_gain).astype(jnp.bfloat16)

    def project(weight):
        return to_sequences(jnp.dot(normed, weight, preferred_element_type=jnp.float32).astype(jnp.bfloat16))
    pieces = tuple((project(weight) for weight in (query_weight, key_weight, value_weight, rec_query_weight, rec_forget_weight, rec_input_weight)))
    scales = to_sequences(forget_scale[:, None])[:, :, 0]

    def per_sequence(inputs):
        q_seq, k_seq, v_seq, rq_seq, rf_seq, ri_seq, scale_seq = inputs
        att_rows, log_sums = attend_sequence(q_seq, k_seq, v_seq, mix_lambda, att_gain)
        rec_rows = recur_sequence(rq_seq, rf_seq, ri_seq, scale_seq, lower_bound, recurrence_gain)
        return (att_rows, rec_rows, log_sums)
    att_all, rec_all, log_all = lax.map(per_sequence, pieces + (scales,))
    att_all = from_sequences(att_all)
    rec_all = from_sequences(rec_all)
    log_weight_sum = from_sequences(log_all.transpose(0, 2, 1)).transpose(1, 0)
    group_width = HEADS * DV // N_TP
    mixed = jnp.zeros((TOKEN_COUNT_ALL, D), jnp.float32)
    for group in range(N_TP):
        lower_col = group * group_width
        upper_col = lower_col + group_width
        portion = jnp.dot(att_all[:, lower_col:upper_col], att_out_weight[lower_col:upper_col], preferred_element_type=jnp.float32)
        portion = portion + jnp.dot(rec_all[:, lower_col:upper_col], rec_out_weight[lower_col:upper_col], preferred_element_type=jnp.float32)
        mixed = mixed + lax.optimization_barrier(portion.astype(jnp.bfloat16)).astype(jnp.float32)
    return (mixed.astype(jnp.bfloat16), log_weight_sum)
```

```python
import functools

import jax
import jax.numpy as jnp
from jax import lax
from jax.experimental import pallas as pl
from jax.experimental.pallas import tpu as pltpu
from jax.sharding import PartitionSpec as P

DK = 64
DV = 128
SUB = 16
EPS = 1e-06
NEG = -1e30
MESH = pl.DeviceIdType.MESH
BF = jnp.bfloat16
F32 = jnp.float32


def dot_nt(a, b):
    return lax.dot_general(a, b, (((1,), (1,)), ((), ())), preferred_element_type=jnp.float32)


def dot_nn(a, b):
    return jnp.dot(a, b, preferred_element_type=jnp.float32)


def grid_of(n_sp):
    ny = 1
    while ny * ny < n_sp:
        ny *= 2
    return n_sp // ny, ny


def kernel(
    n_sp, n_fs, n_tp,
    tok, gain, w0, w1, w2, w3, w4, w5, lam, lower, scale, att_gain, rec_gain, aow, row_w,
    parts, lse,
    aov, rov, wcat, nall, psend, pr, q2, kv2, kvg, qb, osnd, ssnd, orcv, srcv, m_s, l_s, acc,
    smat, olocal, qdec, lsend, lrec, tl, trec, pre, tsnd, rdsnd, zrec, zrd, r3s, s_in,
    w_sem, o_sem, x_s, x_r, f_s, f_r, rel_s, rel_r, b_s, b_r, fo_s, fo_r, kv_s, kv_r, q_s, q_r,
    os_s, os_r, ss_s, ss_r, r1_s, r1_r, r1t_s, r1t_r, r2_s, r2_r, r2t_s, r2t_r, r3_s, r3_r, op_s, op_r,
):
    nz, ny = grid_of(n_sp)
    hz = nz // 2
    sl_rows = DV // ny
    z, f, t = lax.axis_index("sp"), lax.axis_index("fs"), lax.axis_index("tp")
    i, j = z // ny, lax.rem(z, ny)
    mir = nz - 1 - i
    low = jnp.minimum(i, mir)
    hd = jnp.where(i < hz, 0, 1)
    rows, width = tok.shape
    half = rows // n_tp
    quart = half // 2
    heads = n_fs // 2
    right, left = lax.rem(f + 1, n_fs), lax.rem(f + n_fs - 1, n_fs)
    across = lax.rem(f + 2, n_fs)
    j_r, j_l = lax.rem(j + 1, ny), lax.rem(j + ny - 1, ny)

    def remote(src, dst, s, r, **dev):
        return pltpu.make_async_remote_copy(src, dst, s, r, device_id=dev, device_id_type=MESH)

    def sp_of(a, b):
        return a * ny + b

    wcopies = [
        pltpu.make_async_copy(w, wcat.at[pl.ds(n * DK, DK)], w_sem.at[n])
        for n, w in enumerate((w0, w1, w2, w3, w4, w5))
    ]
    for c in wcopies:
        c.start()
    ocopies = [
        pltpu.make_async_copy(aow, aov, o_sem.at[0]),
        pltpu.make_async_copy(row_w, rov, o_sem.at[1]),
    ]

    barrier = pltpu.get_barrier_semaphore()
    for d in range(1, n_fs):
        pl.semaphore_signal(barrier, inc=1, device_id={"fs": lax.rem(f + d, n_fs)}, device_id_type=MESH)
    for d in range(1, n_tp):
        pl.semaphore_signal(barrier, inc=1, device_id={"tp": lax.rem(t + d, n_tp)}, device_id_type=MESH)
    for d in range(1, ny):
        pl.semaphore_signal(barrier, inc=1, device_id={"sp": sp_of(i, lax.rem(j + d, ny))}, device_id_type=MESH)
    for d in range(1, nz):
        pl.semaphore_signal(barrier, inc=1, device_id={"sp": sp_of(lax.rem(i + d, nz), j)}, device_id_type=MESH)

    blk = 32

    @pl.loop(0, rows // blk)
    def _(n):
        sl = pl.ds(pl.multiple_of(n * blk, blk), blk)
        x = tok[sl, :].astype(F32)
        ms = jnp.mean(x * x, axis=-1, keepdims=True)
        nall[0, sl, :] = (x * lax.rsqrt(ms + EPS) * gain[...]).astype(BF)

    st_row = lax.broadcasted_iota(jnp.int32, (8, DV), 0)
    for k in range(1, hz):
        @pl.when(k > i)
        def _():
            for a in (k, nz - 1 - k):
                orcv[a] = jnp.zeros((2, rows, DV), BF)
                srcv[a] = jnp.where(st_row < 2, NEG, 0.0)
    for a in range(nz):
        @pl.when(i <= a)
        def _():
            zrec[a] = jnp.zeros((heads, sl_rows, DV), BF)
            zrd[a] = jnp.ones((heads, DV), F32)

    pl.semaphore_wait(barrier, n_fs - 1 + n_tp - 1 + ny - 1 + nz - 1)

    def pc(n):
        return pl.ds(pl.multiple_of(t * half + n * quart, quart), quart)

    x_a = remote(nall.at[0, pc(0)], nall.at[1, pc(0)], x_s.at[0], x_r.at[0], fs=right)
    x_b = remote(nall.at[0, pc(1)], nall.at[2, pc(1)], x_s.at[1], x_r.at[1], fs=left)
    x_c = remote(nall.at[0, pc(1)], nall.at[1, pc(1)], x_s.at[2], x_r.at[2], fs=right)
    x_d = remote(nall.at[0, pc(0)], nall.at[2, pc(0)], x_s.at[3], x_r.at[3], fs=left)
    f_a = remote(nall.at[1, pc(0)], nall.at[3, pc(0)], f_s.at[0], f_r.at[0], fs=right)
    f_b = remote(nall.at[2, pc(1)], nall.at[3, pc(1)], f_s.at[1], f_r.at[1], fs=left)
    for c in (x_a, x_b, x_c, x_d):
        c.start()
    for c in ocopies:
        c.start()

    relays = []

    def relay(slot, n, idx):
        for e in range(1, n_tp):
            c = remote(
                nall.at[slot, pc(n)], nall.at[slot, pc(n)], rel_s.at[e - 1, idx], rel_r.at[e - 1, idx],
                tp=lax.rem(t + e, n_tp),
            )
            c.start()
            relays.append(c)

    def relay_wait(slot, n, idx):
        for e in range(1, n_tp):
            oth = lax.rem(t + n_tp - e, n_tp)
            sl = pl.ds(pl.multiple_of(oth * half + n * quart, quart), quart)
            remote(
                nall.at[slot, sl], nall.at[slot, sl], rel_s.at[e - 1, idx], rel_r.at[e - 1, idx],
                tp=lax.rem(t + e, n_tp),
            ).wait_recv()

    def project(slot):
        return dot_nt(nall[slot], wcat[...]).astype(BF)

    for c in wcopies:
        c.wait()
    own = project(0)
    for g in range(3):
        pr[f, g] = own[:, g * DV: (g + 1) * DV]

    x_a.wait_recv()
    f_a.start()
    relay(1, 0, 0)
    x_b.wait_recv()
    f_b.start()
    relay(2, 1, 1)
    x_c.wait_recv()
    relay(1, 1, 2)
    x_d.wait_recv()
    relay(2, 0, 3)

    back = (left, right, across)
    res = [
        remote(psend.at[n], pr.at[f], b_s.at[n], b_r.at[n], fs=back[n]) for n in range(3)
    ]

    def deliver(slot):
        got = project(slot)
        for g in range(3):
            psend[slot - 1, g] = got[:, g * DV: (g + 1) * DV]
        res[slot - 1].start()

    relay_wait(1, 0, 0)
    relay_wait(1, 1, 2)
    deliver(1)
    relay_wait(2, 1, 1)
    relay_wait(2, 0, 3)
    deliver(2)
    f_a.wait_recv()
    relay(3, 0, 4)
    f_b.wait_recv()
    relay(3, 1, 5)
    relay_wait(3, 0, 4)
    relay_wait(3, 1, 5)
    deliver(3)

    came = (right, left, across)
    for n in range(3):
        remote(psend.at[n], pr.at[came[n]], b_s.at[n], b_r.at[n], fs=back[n]).wait_recv()

    def pair(h, g, lo):
        return jnp.concatenate([pr[2 * h, g, :, lo: lo + DK], pr[2 * h + 1, g, :, lo: lo + DK]], axis=1)

    for h in range(heads):
        kv2[h, :, :DV] = pair(h, 0, DK)
        kv2[h, :, DV:] = pair(h, 1, 0)
        q2[h] = (pair(h, 0, 0).astype(F32) * DK ** (-0.5)).astype(BF)

    fold = remote(kv2.at[1 - hd], kvg.at[1, j], fo_s, fo_r, sp=sp_of(mir, j))
    fold.start()
    kvg[0, j] = kv2[hd]
    qb[i] = q2[hd]

    right_hops = (ny // 2, ny - 1 - ny // 2)
    left_hops = (ny - 1 - ny // 2, ny // 2)

    def ring(g, way, d):
        y = lax.rem(j + (d if way else ny - d), ny)
        return remote(
            kvg.at[g, y], kvg.at[g, y], kv_s.at[g, way, d], kv_r.at[g, way, d],
            sp=sp_of(i, j_l if way else j_r),
        )

    def ring_wait(g, way, d):
        y = lax.rem(j + (d + 1 if way else ny - d - 1), ny)
        remote(
            kvg.at[g, y], kvg.at[g, y], kv_s.at[g, way, d], kv_r.at[g, way, d],
            sp=sp_of(i, j_l if way else j_r),
        ).wait_recv()

    hops = [(right_hops[g], left_hops[g]) for g in range(2)]

    def step(g, d):
        for way in range(2):
            if 0 < d <= hops[g][way]:
                ring_wait(g, way, d - 1)
            if d < hops[g][way]:
                ring(g, way, d).start()

    step(0, 0)

    def q_copy(a):
        return remote(q2.at[0 if a < hz else 1], qb.at[i], q_s.at[a], q_r.at[i], sp=sp_of(a, j))

    def wanted(a):
        return (min(a, nz - 1 - a) <= i) & (i != a)

    for a in range(nz):
        @pl.when(wanted(a))
        def _():
            q_copy(a).start()

    ri_row = lax.broadcasted_iota(jnp.int32, (rows, DV), 0)
    lane = lax.broadcasted_iota(jnp.int32, (rows, DV), 1)
    sub_pos = lax.rem(ri_row, SUB)
    tri = (
        lax.broadcasted_iota(jnp.int32, (rows, rows), 0)
        >= lax.broadcasted_iota(jnp.int32, (rows, rows), 1)
    )
    trif = tri.astype(F32)
    sc = jnp.broadcast_to(scale[...], (DV, rows)).T
    gates = []
    for h in range(heads):
        rf = pair(h, 2, 0).astype(F32)
        ri = pair(h, 2, DK).astype(F32)
        lb = lower[h: h + 1, :]
        g = sc * jnp.log(lb + (1.0 - lb) * jax.nn.sigmoid(rf))
        kk = 1.0 - jnp.exp(g)
        a = jnp.dot(trif, g, preferred_element_type=F32, precision=lax.Precision.HIGHEST)
        last = a[rows - 1: rows, :]
        kd = (kk * jnp.exp(last - a)).astype(BF)
        lsend[h] = dot_nn(ri.T.astype(BF), kd).astype(BF)
        tl[h: h + 1, :] = jnp.exp(last)
        gates.append((a, kk, ri))

    def sl_of(y):
        return pl.ds(pl.multiple_of(y * sl_rows, sl_rows), sl_rows)

    def r1(d):
        y = lax.rem(j + d, ny)
        return (
            remote(lsend.at[:, sl_of(y)], lrec.at[j], r1_s.at[d], r1_r.at[d], sp=sp_of(i, y)),
            remote(tl, trec.at[j], r1t_s.at[d], r1t_r.at[d], sp=sp_of(i, y)),
        )

    def r1_wait(d):
        y = lax.rem(j + ny - d, ny)
        to = sp_of(i, lax.rem(j + d, ny))
        remote(lsend.at[:, sl_of(j)], lrec.at[y], r1_s.at[d], r1_r.at[d], sp=to).wait_recv()
        remote(tl, trec.at[y], r1t_s.at[d], r1t_r.at[d], sp=to).wait_recv()

    lrec[j] = lsend[:, sl_of(j), :]
    trec[j] = tl[...]
    for d in range(1, ny):
        for c in r1(d):
            c.start()

    fold.wait_recv()
    step(1, 0)
    step(0, 1)

    def local(h):
        a, kk, ri = gates[h]
        rq = pair(h, 1, DK).astype(F32)
        qdec[h] = (rq * jnp.exp(a)).astype(BF)
        smat[h, 0:SUB, :] = jnp.zeros((SUB, rows), BF)
        for n in range(1, rows // SUB):
            lo = n * SUB
            ref = a[lo - 1: lo, :]
            qd = (rq[lo: lo + SUB] * jnp.exp(a[lo: lo + SUB] - ref)).astype(BF)
            kd = (kk * jnp.exp(jnp.where(ri_row < lo, ref - a, NEG))).astype(BF)
            smat[h, lo: lo + SUB, :] = dot_nt(qd, kd).astype(BF)
        o = dot_nn(smat[h], ri.astype(BF))
        o = o + jnp.sum(rq * kk, axis=-1, keepdims=True) * ri
        for d in range(1, SUB):
            valid = sub_pos >= d
            dec = jnp.exp(jnp.where(valid, a - pltpu.roll(a, d, 0), NEG))
            col = jnp.sum(rq * dec * pltpu.roll(kk, d, 0), axis=-1, keepdims=True)
            o = o + col * pltpu.roll(ri, d, 0)
        olocal[h] = o

    local(0)
    step(1, 1)
    step(0, 2)

    for d in range(1, ny):
        r1_wait(d)
    run = jnp.zeros((heads, sl_rows, DV), F32)
    rd = jnp.ones((heads, DV), F32)
    for y in range(ny):
        pre[y] = run
        run = trec[y][:, None, :] * run + lrec[y].astype(F32)
        rd = rd * trec[y]
    tsnd[...] = run.astype(BF)
    rdsnd[...] = rd

    def r2(a):
        return (
            remote(tsnd, zrec.at[i], r2_s.at[a], r2_r.at[i], sp=sp_of(a, j)),
            remote(rdsnd, zrd.at[i], r2t_s.at[a], r2t_r.at[i], sp=sp_of(a, j)),
        )

    def r2_wait(a):
        to = sp_of(lax.rem(i + 1, nz), j)
        remote(tsnd, zrec.at[a], r2_s.at[a], r2_r.at[a], sp=to).wait_recv()
        remote(rdsnd, zrd.at[a], r2t_s.at[a], r2t_r.at[a], sp=to).wait_recv()

    for a in range(1, nz):
        @pl.when(a > i)
        def _():
            for c in r2(a):
                c.start()

    local(1)
    for d in range(1, ny // 2 + 1):
        if d > 1:
            step(1, d)
        if d > 2:
            step(0, d)

    for a in range(nz - 1):
        @pl.when(a < i)
        def _():
            r2_wait(a)
    run = jnp.zeros((heads, sl_rows, DV), F32)
    for a in range(nz - 1):
        run = zrd[a][:, None, :] * run + zrec[a].astype(F32)
    for y in range(ny):
        r3s[y] = (run + pre[y]).astype(BF)
        run = trec[y][:, None, :] * run

    def r3(d):
        y = lax.rem(j + d, ny)
        return remote(r3s.at[y], s_in.at[:, sl_of(j)], r3_s.at[d], r3_r.at[d], sp=sp_of(i, y))

    def r3_wait(d):
        y = lax.rem(j + ny - d, ny)
        to = sp_of(i, lax.rem(j + d, ny))
        remote(r3s.at[y], s_in.at[:, sl_of(y)], r3_s.at[d], r3_r.at[d], sp=to).wait_recv()

    s_in[:, sl_of(j), :] = r3s[j]
    for d in range(1, ny):
        r3(d).start()

    for a in range(nz):
        @pl.when((a >= low) & (i != a))
        def _():
            remote(q2.at[0], qb.at[a], q_s.at[a], q_r.at[a], sp=sp_of(lax.rem(i + 1, nz), j)).wait_recv()

    keys = ny * rows
    off = (
        lax.broadcasted_iota(jnp.int32, (rows, keys), 1)
        - lax.broadcasted_iota(jnp.int32, (rows, keys), 0)
    )

    def strip(b, g, masked):
        q = qb[b]
        kt = kvg[g, :, :, :DV].reshape(keys, DV)
        vt = kvg[g, :, :, DV:].reshape(keys, DV)
        for m in range(2):
            qm = jnp.where((lane < DK) if m == 0 else (lane >= DK), q, jnp.zeros_like(q))
            sco = dot_nt(qm, kt)
            if masked:
                sco = jnp.where(off <= j * rows, sco, NEG)
            old = m_s[m]
            top = jnp.maximum(old, jnp.max(sco, axis=-1, keepdims=True))
            e = jnp.exp(sco - top)
            shrink = jnp.exp(old - top)
            l_s[m] = l_s[m] * shrink + jnp.sum(e, axis=-1, keepdims=True)
            acc[m] = acc[m] * shrink + dot_nn(e.astype(BF), vt)
            m_s[m] = top

    def out_copies(b):
        to = sp_of(b, j)
        return (
            remote(osnd.at[b], orcv.at[i], os_s.at[b], os_r.at[i], sp=to),
            remote(ssnd.at[b], srcv.at[i], ss_s.at[b], ss_r.at[i], sp=to),
        )

    @pl.loop(0, nz - low)
    def _(n):
        b = nz - 1 - n
        m_s[...] = jnp.full(m_s.shape, NEG, F32)
        l_s[...] = jnp.zeros(l_s.shape, F32)
        acc[...] = jnp.zeros(acc.shape, F32)

        @pl.loop(0, 2)
        def _(g):
            row = jnp.where(g == 0, i, mir)

            @pl.when(b == row)
            def _():
                strip(b, g, True)

            @pl.when(b > row)
            def _():
                strip(b, g, False)

        st = jnp.zeros((rows, DV), F32)
        for m in range(2):
            st = jnp.where(lane == m, m_s[m], st)
            st = jnp.where(lane == 2 + m, l_s[m], st)
        st = st.T[:8, :]

        @pl.when(b == i)
        def _():
            for m in range(2):
                orcv[i, m] = acc[m].astype(BF)
            srcv[i] = st

        @pl.when(b != i)
        def _():
            for m in range(2):
                osnd[b, m] = acc[m].astype(BF)
            ssnd[b] = st
            for c in out_copies(b):
                c.start()

    for d in range(1, ny):
        r3_wait(d)
    recs = []
    rg = rec_gain[...]
    for h in range(heads):
        o = olocal[h] + dot_nt(qdec[h], s_in[h])
        ms = jnp.mean(o * o, axis=-1, keepdims=True)
        recs.append((o * lax.rsqrt(ms + EPS) * rg).astype(BF))
    rec = jnp.concatenate(recs, axis=1)
    for c in ocopies:
        c.wait()

    for a in range(nz):
        @pl.when(wanted(a))
        def _():
            to = sp_of(lax.rem(i + 1, nz), j)
            remote(osnd.at[a], orcv.at[a], os_s.at[a], os_r.at[a], sp=to).wait_recv()
            remote(ssnd.at[a], srcv.at[a], ss_s.at[a], ss_r.at[a], sp=to).wait_recv()

    atts = []
    ag = att_gain[...]
    lses = jnp.zeros((rows, DV), F32)
    for h in range(heads):
        src = [k if h == 0 else nz - 1 - k for k in range(hz)]
        st = jnp.concatenate(
            [srcv[a] for a in src] + [jnp.zeros((DV - 8 * hz, DV), F32)], axis=0
        ).T
        outs = []
        for m in range(2):
            tops = [st[:, 8 * k + m: 8 * k + m + 1] for k in range(hz)]
            tots = [st[:, 8 * k + 2 + m: 8 * k + 3 + m] for k in range(hz)]
            top = tops[0]
            for x in tops[1:]:
                top = jnp.maximum(top, x)
            total = jnp.zeros((rows, 1), F32)
            num = jnp.zeros((rows, DV), F32)
            for k in range(hz):
                wk = jnp.exp(tops[k] - top)
                total = total + wk * tots[k]
                num = num + wk * orcv[src[k], m].astype(F32)
            outs.append(num / total)
            if m == 0:
                lses = jnp.where(lane == h, top + jnp.log(total), lses)
        x = outs[0] - lam[0, h] * outs[1]
        ms = jnp.mean(x * x, axis=-1, keepdims=True)
        atts.append((x * lax.rsqrt(ms + EPS) * ag * 0.8).astype(BF))
    lse[...] = lses.T[:heads, :]
    att = jnp.concatenate(atts, axis=1)

    pieces = 4
    cols = width // pieces
    swaps = []
    for n in range(pieces):
        sl = slice(n * cols, (n + 1) * cols)
        parts[0, :, sl] = (dot_nn(att, aov[:, sl]) + dot_nn(rec, rov[:, sl])).astype(BF)
        for e in range(1, n_tp):
            c = remote(
                parts.at[0, :, sl], parts.at[e, :, sl], op_s.at[e - 1, n], op_r.at[e - 1, n],
                tp=lax.rem(t + e, n_tp),
            )
            c.start()
            swaps.append(c)

    for c in (x_a, x_b, x_c, x_d, f_a, f_b, *relays, *res, fold):
        c.wait_send()
    for g in range(2):
        for way in range(2):
            for d in range(hops[g][way]):
                ring(g, way, d).wait_send()
    for d in range(1, ny):
        for c in (*r1(d), r3(d)):
            c.wait_send()
    for a in range(nz):
        @pl.when(wanted(a))
        def _():
            q_copy(a).wait_send()

        @pl.when(a > i)
        def _():
            for c in r2(a):
                c.wait_send()

        @pl.when((a >= low) & (i != a))
        def _():
            for c in out_copies(a):
                c.wait_send()
    for c in swaps:
        c.wait()


def finish(parts, lse_in, mixed, lse):
    total = parts[0].astype(jnp.float32)
    for e in range(1, parts.shape[0]):
        total = total + parts[e].astype(jnp.float32)
    mixed[...] = total.astype(jnp.bfloat16)
    lse[...] = lse_in[...]


def solution(mesh):
    n_sp, n_fs, n_tp = (mesh.shape[k] for k in ("sp", "fs", "tp"))
    nz, ny = grid_of(n_sp)

    def on_device(
        tokens, in_gain, wq, wk, wvv, wrq, wrf, wri, lam, lower, scale, att_gain, rec_gain, aow, row_w
    ):
        rows, width = tokens.shape
        heads = lower.shape[0]
        assert heads == 2 and n_fs == 4 and rows == DV and nz % 2 == 0
        vm = pl.BlockSpec(memory_space=pltpu.VMEM)
        sm = pl.BlockSpec(memory_space=pltpu.SMEM)
        hbm = pl.BlockSpec(memory_space=pl.ANY)
        dma = pltpu.SemaphoreType.DMA
        peers = n_fs - 1
        pieces = 4
        slr = DV // ny
        hmax = max(ny // 2, 1)
        parts, lse = pl.pallas_call(
            functools.partial(kernel, n_sp, n_fs, n_tp),
            out_shape=(
                jax.ShapeDtypeStruct((n_tp, rows, width), BF),
                jax.ShapeDtypeStruct((heads, rows), F32),
            ),
            in_specs=[vm, vm] + [hbm] * 6 + [sm, vm, vm, vm, vm, hbm, hbm],
            out_specs=(vm, vm),
            scratch_shapes=[
                pltpu.VMEM(aow.shape, BF),
                pltpu.VMEM(row_w.shape, BF),
                pltpu.VMEM((6 * DK, width), BF),
                pltpu.VMEM((n_fs, rows, width), BF),
                pltpu.VMEM((peers, 3, rows, DV), BF),
                pltpu.VMEM((n_fs, 3, rows, DV), BF),
                pltpu.VMEM((heads, rows, DV), BF),
                pltpu.VMEM((heads, rows, 2 * DV), BF),
                pltpu.VMEM((2, ny, rows, 2 * DV), BF),
                pltpu.VMEM((nz, rows, DV), BF),
                pltpu.VMEM((nz, 2, rows, DV), BF),
                pltpu.VMEM((nz, 8, DV), F32),
                pltpu.VMEM((nz, 2, rows, DV), BF),
                pltpu.VMEM((nz, 8, DV), F32),
                pltpu.VMEM((2, rows, 1), F32),
                pltpu.VMEM((2, rows, 1), F32),
                pltpu.VMEM((2, rows, DV), F32),
                pltpu.VMEM((heads, rows, rows), BF),
                pltpu.VMEM((heads, rows, DV), F32),
                pltpu.VMEM((heads, rows, DV), BF),
                pltpu.VMEM((heads, DV, DV), BF),
                pltpu.VMEM((ny, heads, slr, DV), BF),
                pltpu.VMEM((heads, DV), F32),
                pltpu.VMEM((ny, heads, DV), F32),
                pltpu.VMEM((ny, heads, slr, DV), F32),
                pltpu.VMEM((heads, slr, DV), BF),
                pltpu.VMEM((heads, DV), F32),
                pltpu.VMEM((nz, heads, slr, DV), BF),
                pltpu.VMEM((nz, heads, DV), F32),
                pltpu.VMEM((ny, heads, slr, DV), BF),
                pltpu.VMEM((heads, DV, DV), BF),
                dma((6,)), dma((2,)),
                dma((4,)), dma((4,)), dma((2,)), dma((2,)),
                dma((max(n_tp - 1, 1), 6)), dma((max(n_tp - 1, 1), 6)),
                dma((peers,)), dma((peers,)),
                dma, dma,
                dma((2, 2, hmax)), dma((2, 2, hmax)),
                dma((nz,)), dma((nz,)),
                dma((nz,)), dma((nz,)), dma((nz,)), dma((nz,)),
                dma((ny,)), dma((ny,)), dma((ny,)), dma((ny,)),
                dma((nz,)), dma((nz,)), dma((nz,)), dma((nz,)),
                dma((ny,)), dma((ny,)),
                dma((max(n_tp - 1, 1), pieces)), dma((max(n_tp - 1, 1), pieces)),
            ],
            compiler_params=pltpu.CompilerParams(
                collective_id=0, has_side_effects=True, vmem_limit_bytes=56 * 1024 * 1024
            ),
            name="mixer",
        )(
            tokens, in_gain[None], wq.T, wk.T, wvv.T, wrq.T, wrf.T, wri.T, lam[None], lower, scale[None],
            att_gain[None], rec_gain[None], aow, row_w,
        )
        half = width // 2
        return pl.pallas_call(
            finish,
            grid=(2,),
            out_shape=(
                jax.ShapeDtypeStruct((rows, width), BF),
                jax.ShapeDtypeStruct((heads, rows), F32),
            ),
            in_specs=[
                pl.BlockSpec((n_tp, rows, half), lambda n: (0, 0, n)),
                pl.BlockSpec((heads, rows), lambda n: (0, 0)),
            ],
            out_specs=(
                pl.BlockSpec((rows, half), lambda n: (0, n)),
                pl.BlockSpec((heads, rows), lambda n: (0, 0)),
            ),
            name="finish",
        )(parts, lse)

    col = P(None, ("tp", "fs"))
    return jax.shard_map(
        on_device,
        mesh=mesh,
        in_specs=(
            P(("fs", "sp"), None), P(), col, col, col, col, col, col,
            P("tp"), P("tp", None), P(("fs", "sp")), P(), P(), P("tp", None), P("tp", None),
        ),
        out_specs=(P(("fs", "sp"), None), P("tp", ("fs", "sp"))),
        check_vma=False,
    )
```

```python
import functools

import jax
import jax.numpy as jnp
from jax import lax
from jax.experimental import pallas as pl
from jax.experimental.pallas import tpu as pltpu
from jax.sharding import PartitionSpec as P

DK = 64
DV = 128
SUB = 16
EPS = 1e-06
NEG = -1e30
MESH = pl.DeviceIdType.MESH
BF = jnp.bfloat16
F32 = jnp.float32


def dot_nt(a, b):
    return lax.dot_general(a, b, (((1,), (1,)), ((), ())), preferred_element_type=jnp.float32)


def dot_nn(a, b):
    return jnp.dot(a, b, preferred_element_type=jnp.float32)


def grid_of(n_sp):
    ny = 1
    while ny * ny < n_sp:
        ny *= 2
    return n_sp // ny, ny


def kernel(
    n_sp, n_fs, n_tp,
    tok, gain_h, w0, w1, w2, w3, w4, w5, lam_h, lower_h, scale_h, att_gain_h, rec_gain_h, aow, row_w,
    parts, lse,
    tokv, gain, lam, lower, scale, att_gain, rec_gain, aov, rov, wcat, nown, near_a, near_c, far, psend, pr, kvp, q2, kvg, qb,
    osnd, orcv, stx, lsrow, prt, m_s, l_s, acc,
    smat, olocal, qdec, lsend, lrec, tl, trec, pre, tsnd, rdsnd, zrec, zrd, r3s, s_in,
    t_sem, g_sem, w_sem, o_sem, xa_r, xc_r, xf_r, x_s, xf_s, rel_s, rel_r,
    b_s, b_r, c_s, c_r, kp_s, k0_s, kp_r, kv_s, kv_r, q_s, q_r,
    os_s, os_r, sx_s, sx_r, sy_s, sy_r, r1_s, r1_r, r1t_s, r1t_r, r2_s, r2_r, r2t_s, r2t_r, r3_s, r3_r, op_s, op_r,
):
    nz, ny = grid_of(n_sp)
    hz = nz // 2
    sl_rows = DV // ny
    z, f, t = lax.axis_index("sp"), lax.axis_index("fs"), lax.axis_index("tp")
    i, j = z // ny, lax.rem(z, ny)
    mir = nz - 1 - i
    low = jnp.minimum(i, mir)
    hd = jnp.where(i < hz, 0, 1)
    rows, width = tok.shape
    half = rows // n_tp
    qr = half // 2
    hq = qr // 2
    heads = n_fs // 2
    right, left = lax.rem(f + 1, n_fs), lax.rem(f + n_fs - 1, n_fs)
    across = lax.rem(f + 2, n_fs)
    j_r, j_l = lax.rem(j + 1, ny), lax.rem(j + ny - 1, ny)

    def remote(src, dst, s, r, **dev):
        return pltpu.make_async_remote_copy(src, dst, s, r, device_id=dev, device_id_type=MESH)

    def landed(ref, sem):
        pltpu.make_async_copy(ref, ref, sem).wait()

    def sp_of(a, b):
        return a * ny + b

    tcopy = pltpu.make_async_copy(tok, tokv, t_sem)
    tcopy.start()
    scopies = [
        pltpu.make_async_copy(a, b, g_sem.at[n])
        for n, (a, b) in enumerate((
            (gain_h, gain), (lam_h, lam), (lower_h, lower), (scale_h, scale),
            (att_gain_h, att_gain), (rec_gain_h, rec_gain),
        ))
    ]
    for c in scopies:
        c.start()
    barrier = pltpu.get_barrier_semaphore()
    for d in range(1, n_fs):
        peer = lax.rem(f + d, n_fs)
        pl.semaphore_signal(barrier, inc=1, device_id={"fs": peer}, device_id_type=MESH)
        pl.semaphore_signal(
            barrier, inc=1, device_id={"fs": peer, "sp": sp_of(mir, j)}, device_id_type=MESH
        )
    for d in range(1, n_tp):
        pl.semaphore_signal(barrier, inc=1, device_id={"tp": lax.rem(t + d, n_tp)}, device_id_type=MESH)
    for d in range(1, ny):
        pl.semaphore_signal(barrier, inc=1, device_id={"sp": sp_of(i, lax.rem(j + d, ny))}, device_id_type=MESH)
    for d in range(1, nz):
        pl.semaphore_signal(barrier, inc=1, device_id={"sp": sp_of(lax.rem(i + d, nz), j)}, device_id_type=MESH)

    wcopies = [
        pltpu.make_async_copy(w, wcat.at[pl.ds(n * DK, DK)], w_sem)
        for n, w in enumerate((w1, w2, w0, w3, w4, w5))
    ]
    for c in wcopies:
        c.start()
    ocopies = [
        pltpu.make_async_copy(aow, aov, o_sem.at[0]),
        pltpu.make_async_copy(row_w, rov, o_sem.at[1]),
    ]

    blk = 32
    tcopy.wait()
    scopies[0].wait()

    @pl.loop(0, rows // blk)
    def _(n):
        sl = pl.ds(pl.multiple_of(n * blk, blk), blk)
        x = tokv[sl, :].astype(F32)
        ms = jnp.mean(x * x, axis=-1, keepdims=True)
        nown[sl, :] = (x * lax.rsqrt(ms + EPS) * gain[...]).astype(BF)

    m_s[...] = jnp.full(m_s.shape, NEG, F32)
    l_s[...] = jnp.zeros(l_s.shape, F32)
    acc[...] = jnp.zeros(acc.shape, F32)
    for k in range(1, hz):
        @pl.when(k > i)
        def _():
            for h in range(2):
                orcv[h, k] = jnp.zeros((rows, DV), BF)
    pl.semaphore_wait(barrier, 2 * (n_fs - 1) + n_tp - 1 + ny - 1 + nz - 1)

    def own_rows(at, size):
        return nown.at[pl.ds(pl.multiple_of(t * half + at, hq), size)]

    def send_a(way, n):
        return remote(
            own_rows(way * qr + n * hq, hq), near_a.at[way, t, pl.ds(n * hq, hq)],
            x_s, xa_r.at[way, n], fs=left if way else right,
        )

    def send_c(way):
        return remote(
            own_rows((1 - way) * qr, qr), near_c.at[way, t], x_s, xc_r.at[way], fs=left if way else right
        )

    def send_f(way, n):
        at = pl.ds(n * hq, hq)
        return remote(
            near_a.at[way, t, at], far.at[t, way, at], xf_s, xf_r.at[way, n], fs=left if way else right
        )

    for n in range(2):
        for way in range(2):
            send_a(way, n).start()
    for way in range(2):
        send_c(way).start()
    for c in ocopies:
        c.start()

    def relay(idx, at):
        for e in range(1, n_tp):
            remote(at, at, rel_s.at[idx], rel_r.at[idx], tp=lax.rem(t + e, n_tp)).start()

    def relayed(idx, at):
        if n_tp > 1:
            landed(at, rel_r.at[idx])

    oth = n_tp - 1 - t

    def project(x):
        return dot_nt(x.reshape(rows, width), wcat[...]).astype(BF)

    def split(x):
        return x.reshape(n_tp, 2, qr, DV)

    landed(wcat, w_sem)


    back = (f, left, right, across)
    part = lax.rem(f, 2)
    mine = f // 2 == hd
    row_to = jnp.where(mine, i, mir)

    def kv_copy(slot, a):
        return remote(
            psend.at[slot, 0, :, a], kvp.at[hd, part, :, a], kp_s if slot else k0_s, kp_r.at[hd, part, a],
            sp=sp_of(row_to, j), fs=back[slot],
        )

    def q_part(slot, a):
        return remote(psend.at[slot, 1, :, a], pr.at[f, 0, :, a], b_s, b_r, fs=back[slot])

    def r_part(slot, a):
        return remote(psend.at[slot, 2, :, a], pr.at[f, 1, :, a], c_s, c_r, fs=back[slot])

    own = project(nown[...])
    pr[f, 0] = split(own[:, DV: 2 * DV])
    pr[f, 1] = split(own[:, 2 * DV:])

    @pl.when(mine)
    def _():
        kvp[hd, part] = split(own[:, :DV])

    @pl.when(jnp.logical_not(mine))
    def _():
        psend[0, 0] = split(own[:, :DV])
        for a in range(2):
            kv_copy(0, a).start()

    def deliver(todo, rest=()):
        for slot, a in todo:
            kv_copy(slot, a).start()
        for slot, a in rest:
            q_part(slot, a).start()
        for slot, a in rest:
            r_part(slot, a).start()

    def deliver_near(x, flip, rest):
        got = project(x)
        todo = []
        for way in range(2):
            a = 1 - way if flip else way
            for c in range(n_tp):
                lo = (way * n_tp + c) * qr
                for g in range(3):
                    psend[1 + way, g, c, a] = got[lo: lo + qr, g * DV: (g + 1) * DV]
            todo.append((1 + way, a))
        deliver(todo, rest)

    for n in range(2):
        for way in range(2):
            landed(near_a.at[way, t, pl.ds(n * hq, hq)], xa_r.at[way, n])
            send_f(way, n).start()
            relay(0, near_a.at[way, t, pl.ds(n * hq, hq)])
    relayed(0, near_a.at[:, oth])
    deliver_near(near_a[...], False, [])
    for way in range(2):
        landed(near_c.at[way, t], xc_r.at[way])
        relay(2, near_c.at[way, t])
    relayed(2, near_c.at[:, oth])
    deliver_near(near_c[...], True, [(1, 0), (2, 1)])
    for n in range(2):
        for way in range(2):
            landed(far.at[t, way, pl.ds(n * hq, hq)], xf_r.at[way, n])
            relay(1, far.at[t, way, pl.ds(n * hq, hq)])
    relayed(1, far.at[oth])
    far_rows = far[...].reshape(rows, width)
    psend[3, 0] = split(dot_nt(far_rows, wcat[:DV]).astype(BF))
    deliver([(3, 0), (3, 1)])
    got = dot_nt(far_rows, wcat[DV:]).astype(BF)
    for g in range(2):
        psend[3, 1 + g] = split(got[:, g * DV: (g + 1) * DV])
    deliver([], [(3, 0), (3, 1), (1, 1), (2, 0)])

    def flat(x):
        return x.reshape(rows, DV)

    def pair(h, g, lo):
        return jnp.concatenate([flat(pr[2 * h + p, g])[:, lo: lo + DK] for p in range(2)], axis=1)

    slot_of = (hd, 1 - hd)

    def gather_kv(role):
        g = slot_of[role]
        for p in range(2):
            @pl.when((role == 1) | (2 * hd + p != f))
            def _():
                for a in range(2):
                    landed(kvp.at[g, p, :, a], kp_r.at[g, p, a])
        got = [flat(kvp[g, p]) for p in range(2)]
        kvg[g, j, :, :DV] = jnp.concatenate([x[:, :DK] for x in got], axis=1)
        kvg[g, j, :, DV:] = jnp.concatenate([x[:, DK:] for x in got], axis=1)

    right_hops = (ny // 2, ny - 1 - ny // 2)
    left_hops = (ny - 1 - ny // 2, ny // 2)

    half_k = rows // 2

    def block(role, way, d, n):
        return kvg.at[slot_of[role], lax.rem(j + (d if way else ny - d), ny), pl.ds(n * half_k, half_k)]

    def ring(role, way, d, n):
        at = block(role, way, d, n)
        return remote(at, at, kv_s, kv_r.at[role, way, d, n], sp=sp_of(i, j_l if way else j_r))

    hops = [(right_hops[g], left_hops[g]) for g in range(2)]

    taken = set()

    def step(g, d, again=False):
        if (g, d) in taken and not again:
            return
        taken.add((g, d))
        for n in range(2):
            for way in range(2):
                if 0 < d <= hops[g][way]:
                    landed(block(g, way, d, n), kv_r.at[g, way, d - 1, n])
                if d < hops[g][way]:
                    ring(g, way, d, n).start()

    gather_kv(0)
    step(0, 0)
    gather_kv(1)
    step(1, 0)

    landed(pr.at[pl.ds(0, n_fs - 1), 0], b_r)
    for h in range(heads):
        q2[h] = (pair(h, 0, 0).astype(F32) * DK ** (-0.5)).astype(BF)
    qb[i] = q2[hd]

    def q_copy(d):
        a = lax.rem(i + d, nz)
        return remote(q2.at[jnp.where(a < hz, 0, 1)], qb.at[i], q_s, q_r, sp=sp_of(a, j))

    def wanted(a):
        return (min(a, nz - 1 - a) <= i) & (i != a)

    for d in range(1, nz):
        q_copy(d).start()

    landed(pr.at[pl.ds(0, n_fs - 1), 1], c_r)

    ri_row = lax.broadcasted_iota(jnp.int32, (rows, DV), 0)
    lane = lax.broadcasted_iota(jnp.int32, (rows, DV), 1)
    sub_pos = lax.rem(ri_row, SUB)
    tri = (
        lax.broadcasted_iota(jnp.int32, (rows, rows), 0)
        >= lax.broadcasted_iota(jnp.int32, (rows, rows), 1)
    )
    trif = tri.astype(F32)
    gates = []
    for c in scopies[1:]:
        c.wait()
    sc = jnp.broadcast_to(scale[...], (DV, rows)).T
    for h in range(heads):
        rf = pair(h, 1, 0).astype(F32)
        ri = pair(h, 1, DK).astype(F32)
        lb = lower[h: h + 1, :]
        g = sc * jnp.log(lb + (1.0 - lb) * jax.nn.sigmoid(rf))
        kk = 1.0 - jnp.exp(g)
        a = jnp.dot(trif, g, preferred_element_type=F32, precision=lax.Precision.HIGHEST)
        last = a[rows - 1: rows, :]
        kd = (kk * jnp.exp(last - a)).astype(BF)
        lsend[h] = dot_nn(ri.T.astype(BF), kd).astype(BF)
        tl[h: h + 1, :] = jnp.exp(last)
        gates.append((a, kk, ri))

    def sl_of(y):
        return pl.ds(pl.multiple_of(y * sl_rows, sl_rows), sl_rows)

    def r1(d):
        y = lax.rem(j + d, ny)
        return (
            remote(lsend.at[:, sl_of(y)], lrec.at[j], r1_s, r1_r, sp=sp_of(i, y)),
            remote(tl, trec.at[j], r1t_s, r1t_r, sp=sp_of(i, y)),
        )

    lrec[j] = lsend[:, sl_of(j), :]
    trec[j] = tl[...]
    for d in range(1, ny):
        for c in r1(d):
            c.start()

    step(0, 1)
    step(1, 1)

    def local(h):
        a, kk, ri = gates[h]
        rq = pair(h, 0, DK).astype(F32)
        qdec[h] = (rq * jnp.exp(a)).astype(BF)
        smat[h, 0:SUB, :] = jnp.zeros((SUB, rows), BF)
        for n in range(1, rows // SUB):
            lo = n * SUB
            ref = a[lo - 1: lo, :]
            qd = (rq[lo: lo + SUB] * jnp.exp(a[lo: lo + SUB] - ref)).astype(BF)
            kd = (kk * jnp.exp(jnp.where(ri_row < lo, ref - a, NEG))).astype(BF)
            smat[h, lo: lo + SUB, :] = dot_nt(qd, kd).astype(BF)
        o = dot_nn(smat[h], ri.astype(BF))
        o = o + jnp.sum(rq * kk, axis=-1, keepdims=True) * ri
        for d in range(1, SUB):
            valid = sub_pos >= d
            dec = jnp.exp(jnp.where(valid, a - pltpu.roll(a, d, 0), NEG))
            col = jnp.sum(rq * dec * pltpu.roll(kk, d, 0), axis=-1, keepdims=True)
            o = o + col * pltpu.roll(ri, d, 0)
        olocal[h] = o

    local(0)
    local(1)
    diag = (
        lax.broadcasted_iota(jnp.int32, (rows, rows), 1)
        - lax.broadcasted_iota(jnp.int32, (rows, rows), 0)
    )

    def strip(chunk, blocks, groups, offs):
        kts, vts, masks = [], [], []
        for g, masked in groups:
            for o in offs:
                y = lax.rem(j + o, ny)
                kts.append(kvg[g, y, :, :DV])
                vts.append(kvg[g, y, :, DV:])
                masks.append(diag <= (j - y) * rows if masked else None)
        kt = jnp.concatenate(kts, axis=0)
        vt = jnp.concatenate(vts, axis=0)
        scores = []
        for b in blocks:
            q = qb[b]
            for m in range(2):
                scores.append(dot_nt(jnp.where((lane < DK) if m == 0 else (lane >= DK), q, jnp.zeros_like(q)), kt))
        done = []
        for sco in scores:
            if any(x is not None for x in masks):
                sco = jnp.concatenate([
                    sco[:, n * rows: (n + 1) * rows] if x is None
                    else jnp.where(x, sco[:, n * rows: (n + 1) * rows], NEG)
                    for n, x in enumerate(masks)
                ], axis=1)
            top = jnp.max(sco, axis=-1, keepdims=True)
            e = jnp.exp(sco - top)
            done.append((top, jnp.sum(e, axis=-1, keepdims=True), dot_nn(e.astype(BF), vt)))
        for n, (top, tot, num) in enumerate(done):
            b, m = blocks[n // 2], n % 2
            m_s[chunk, b, m] = top
            l_s[chunk, b, m] = tot
            acc[chunk, b, m] = num

    high = nz - 1 - low

    def sweep(chunk, dists, between=None):
        offs = sorted({o % ny for d in dists for o in (d, -d) if d <= ny // 2})
        if not offs:
            return

        strip(chunk, [low], [(0, True)], offs)

        @pl.loop(0, (high - low - 1) // 2)
        def _(n):
            strip(chunk, [low + 1 + 2 * n, low + 2 + 2 * n], [(0, False)], offs)

        if between is not None:
            pl.when(low < hz // 2)(between)
        strip(chunk, [high], [(0, False), (1, True)], offs)
        if between is not None:
            pl.when(low >= hz // 2)(between)

        @pl.loop(high + 1, nz)
        def _(b):
            strip(chunk, [b], [(0, False), (1, False)], offs)

    step(0, 2)
    step(1, 2)

    landed(lrec.at[pl.ds(0, ny - 1)], r1_r)
    landed(trec.at[pl.ds(0, ny - 1)], r1t_r)
    run = jnp.zeros((heads, sl_rows, DV), F32)
    rd = jnp.ones((heads, DV), F32)
    for y in range(ny):
        pre[y] = run
        run = trec[y][:, None, :] * run + lrec[y].astype(F32)
        rd = rd * trec[y]
    tsnd[...] = run.astype(BF)
    rdsnd[...] = rd

    def r2(d):
        to = sp_of(lax.rem(i + d, nz), j)
        return (
            remote(tsnd, zrec.at[i], r2_s, r2_r, sp=to),
            remote(rdsnd, zrd.at[i], r2t_s, r2t_r, sp=to),
        )

    for d in range(1, nz):
        for c in r2(d):
            c.start()

    landed(qb.at[pl.ds(0, nz - 1)], q_r)

    def row_of(h, k):
        return jnp.where(h == 0, k, nz - 1 - k)

    def stat_copy(chunk, d):
        at = stx.at[hd, low, chunk]
        return remote(at, at, sx_s.at[chunk], sx_r.at[chunk], sp=sp_of(row_of(hd, lax.rem(low + d, hz)), j))

    def emit(chunk):
        st = jnp.zeros((rows, DV), F32)
        for b in range(nz):
            for m in range(2):
                st = jnp.where(lane == m * nz + b, m_s[chunk, b, m], st)
                st = jnp.where(lane == (2 + m) * nz + b, l_s[chunk, b, m], st)
        stx[hd, low, chunk] = st.T[:4 * nz, :]
        for d in range(1, hz):
            stat_copy(chunk, d).start()

    def lse_copy(k):
        b = row_of(1 - hd, k)
        return remote(
            lsrow.at[hd, pl.ds(b, 1)], lsrow.at[hd, pl.ds(b, 1)], sy_s, sy_r, sp=sp_of(b, j)
        )

    def out_copy(b):
        return remote(osnd.at[b], orcv.at[hd, low], os_s.at[b], os_r.at[hd, low], sp=sp_of(b, j))

    def third():
        for g in range(2):
            step(g, 3, True)

    sweep(0, (0, 1, 2), between=third)
    emit(0)
    for d in range(3, ny // 2 + 1):
        for g in range(2):
            step(g, d)

    landed(zrec.at[pl.ds(0, nz - 1)], r2_r)
    landed(zrd.at[pl.ds(0, nz - 1)], r2t_r)
    run = jnp.zeros((heads, sl_rows, DV), F32)
    for a in range(nz - 1):
        run = jnp.where(a < i, zrd[a][:, None, :] * run + zrec[a].astype(F32), run)
    for y in range(ny):
        r3s[y] = (run + pre[y]).astype(BF)
        run = trec[y][:, None, :] * run

    def r3(d):
        y = lax.rem(j + d, ny)
        return remote(r3s.at[y], s_in.at[:, sl_of(j)], r3_s, r3_r, sp=sp_of(i, y))

    s_in[:, sl_of(j), :] = r3s[j]
    for d in range(1, ny):
        r3(d).start()

    sweep(1, range(3, ny // 2 + 1))
    emit(1)

    lam_h = jnp.where(hd == 0, lam[0, 0], lam[0, 1])

    def send_out(b, num):
        @pl.when(b == i)
        def _():
            orcv[hd, low] = num

        @pl.when(b != i)
        def _():
            osnd[b] = num
            out_copy(b).start()

    @pl.when(low == 0)
    def _():
        weights = []
        for m in range(2):
            tops = [stx[hd, 0, chunk, m * nz: m * nz + 1, :] for chunk in range(2)]
            tots = [stx[hd, 0, chunk, (2 + m) * nz: (2 + m) * nz + 1, :] for chunk in range(2)]
            top = jnp.maximum(tops[0], tops[1])
            scales = [jnp.exp(x - top) for x in tops]
            total = scales[0] * tots[0] + scales[1] * tots[1]
            for x in scales:
                weights.append(-lam_h * (x / total) if m else x / total)
        wt = jnp.concatenate(weights + [jnp.zeros((DV - 4, DV), F32)], axis=0).T
        num = jnp.zeros((rows, DV), F32)
        for m in range(2):
            for chunk in range(2):
                at = 2 * m + chunk
                num = num + acc[chunk, 0, m] * wt[:, at: at + 1]
        send_out(0, num.astype(BF))

    landed(r3s.at[pl.ds(0, ny - 1)], r3_r)
    recs = []
    rg = rec_gain[...]
    for h in range(heads):
        o = olocal[h] + dot_nt(qdec[h], s_in[h])
        ms = jnp.mean(o * o, axis=-1, keepdims=True)
        recs.append((o * lax.rsqrt(ms + EPS) * rg).astype(BF))
    rec = jnp.concatenate(recs, axis=1)
    for c in ocopies:
        c.wait()
    pieces = 4
    cols = width // pieces
    for n in range(pieces):
        sl = slice(n * cols, (n + 1) * cols)
        prt[:, sl] = dot_nn(rec, rov[:, sl])

    if hz > 1:
        for chunk in range(2):
            landed(stx.at[0, pl.ds(0, hz - 1), chunk], sx_r.at[chunk])

    def stat(k, chunk, r):
        return stx[hd, k, chunk, r * nz: (r + 1) * nz, :]

    sources = [(k, chunk) for k in range(hz) for chunk in range(2)]
    weights = []
    for m in range(2):
        top = stat(0, 0, m)
        for k, chunk in sources[1:]:
            top = jnp.maximum(top, stat(k, chunk, m))
        total = jnp.zeros((nz, DV), F32)
        for k, chunk in sources:
            total = total + jnp.exp(stat(k, chunk, m) - top) * stat(k, chunk, 2 + m)
        if m == 0:
            lsrow[hd] = top + jnp.log(total)
        for chunk in range(2):
            wt = jnp.exp(stx[hd, low, chunk, pl.ds(m * nz, nz), :] - top) / total
            weights.append(-lam_h * wt if m else wt)

    @pl.when(low == 0)
    def _():
        for k in range(hz):
            lse_copy(k).start()

    wt = jnp.concatenate(weights + [jnp.zeros((DV - 4 * nz, DV), F32)], axis=0).T
    for b in range(1, nz):
        @pl.when(b >= low)
        def _():
            num = jnp.zeros((rows, DV), F32)
            for m in range(2):
                for chunk in range(2):
                    at = (2 * m + chunk) * nz + b
                    num = num + acc[chunk, b, m] * wt[:, at: at + 1]
            send_out(b, num.astype(BF))

    landed(lsrow.at[0, pl.ds(0, 1)], sy_r)
    for k in range(hz):
        for h in range(2):
            @pl.when((k <= i) & ((hd != h) | (low != k)))
            def _():
                landed(orcv.at[h, k], os_r.at[h, k])

    atts = []
    ag = att_gain[...]
    for h in range(heads):
        lse[h: h + 1, :] = lsrow[h, pl.ds(i, 1), :]
        x = orcv[h, 0].astype(F32)
        for k in range(1, hz):
            x = x + orcv[h, k].astype(F32)
        ms = jnp.mean(x * x, axis=-1, keepdims=True)
        atts.append((x * lax.rsqrt(ms + EPS) * ag * 0.8).astype(BF))
    att = jnp.concatenate(atts, axis=1)

    for n in range(pieces):
        sl = slice(n * cols, (n + 1) * cols)
        parts[0, :, sl] = (dot_nn(att, aov[:, sl]) + prt[:, sl]).astype(BF)
        for e in range(1, n_tp):
            c = remote(
                parts.at[0, :, sl], parts.at[e, :, sl], op_s, op_r,
                tp=lax.rem(t + e, n_tp),
            )
            c.start()

    landed(nown, x_s)
    landed(near_a.at[:, 0], xf_s)
    if n_tp > 1:
        landed(near_a.at[:, 0], rel_s.at[0])
        landed(far.at[0], rel_s.at[1])
        landed(near_c.at[:, 0], rel_s.at[2])
    landed(psend.at[pl.ds(1, n_fs - 1), 0], kp_s)
    landed(psend.at[pl.ds(1, n_fs - 1), 1], b_s)
    landed(psend.at[pl.ds(1, n_fs - 1), 2], c_s)

    @pl.when(jnp.logical_not(mine))
    def _():
        landed(psend.at[0, 0], k0_s)

    landed(kvg.at[:, pl.ds(0, ny - 1)], kv_s)
    landed(qb.at[pl.ds(0, nz - 1)], q_s)
    landed(lrec.at[pl.ds(0, ny - 1)], r1_s)
    landed(trec.at[pl.ds(0, ny - 1)], r1t_s)
    landed(zrec.at[pl.ds(0, nz - 1)], r2_s)
    landed(zrd.at[pl.ds(0, nz - 1)], r2t_s)
    landed(r3s.at[pl.ds(0, ny - 1)], r3_s)
    if hz > 1:
        for chunk in range(2):
            landed(stx.at[0, pl.ds(0, hz - 1), chunk], sx_s.at[chunk])

    @pl.when(low == 0)
    def _():
        landed(lsrow.at[0, pl.ds(0, hz)], sy_s)

    for a in range(nz):
        @pl.when((a >= low) & (i != a))
        def _():
            out_copy(a).wait_send()
    if n_tp > 1:
        landed(parts.at[0], op_s)
        landed(parts.at[1], op_r)


def finish(parts, lse_in, mixed, lse):
    total = parts[0].astype(jnp.float32)
    for e in range(1, parts.shape[0]):
        total = total + parts[e].astype(jnp.float32)
    mixed[...] = total.astype(jnp.bfloat16)
    lse[...] = lse_in[...]


def solution(mesh):
    n_sp, n_fs, n_tp = (mesh.shape[k] for k in ("sp", "fs", "tp"))
    nz, ny = grid_of(n_sp)

    def on_device(
        tokens, in_gain, wq, wk, wvv, wrq, wrf, wri, lam, lower, scale, att_gain, rec_gain, aow, row_w
    ):
        rows, width = tokens.shape
        heads = lower.shape[0]
        assert heads == 2 and n_fs == 4 and rows == DV and nz % 2 == 0
        vm = pl.BlockSpec(memory_space=pltpu.VMEM)
        hbm = pl.BlockSpec(memory_space=pltpu.HBM)
        dma = pltpu.SemaphoreType.DMA
        qr = rows // (2 * n_tp)
        slr = DV // ny
        hmax = max(ny // 2, 1)
        parts, lse = pl.pallas_call(
            functools.partial(kernel, n_sp, n_fs, n_tp),
            out_shape=(pltpu.VMEM((n_tp, rows, width), BF), pltpu.VMEM((heads, rows), F32)),
            in_specs=[hbm] * 15,
            out_specs=(vm, vm),
            scratch_shapes=[
                pltpu.VMEM(tokens.shape, BF),
                pltpu.VMEM((1, width), F32),
                pltpu.SMEM((1, heads), F32),
                pltpu.VMEM((heads, DV), F32),
                pltpu.VMEM((1, rows), F32),
                pltpu.VMEM((1, DV), F32),
                pltpu.VMEM((1, DV), F32),
                pltpu.VMEM(aow.shape, BF),
                pltpu.VMEM(row_w.shape, BF),
                pltpu.VMEM((6 * DK, width), BF),
                pltpu.VMEM((rows, width), BF),
                pltpu.VMEM((2, n_tp, qr, width), BF),
                pltpu.VMEM((2, n_tp, qr, width), BF),
                pltpu.VMEM((n_tp, 2, qr, width), BF),
                pltpu.VMEM((n_fs, 3, n_tp, 2, qr, DV), BF),
                pltpu.VMEM((n_fs, 2, n_tp, 2, qr, DV), BF),
                pltpu.VMEM((2, 2, n_tp, 2, qr, DV), BF),
                pltpu.VMEM((heads, rows, DV), BF),
                pltpu.VMEM((2, ny, rows, 2 * DV), BF),
                pltpu.VMEM((nz, rows, DV), BF),
                pltpu.VMEM((nz, rows, DV), BF),
                pltpu.VMEM((2, nz // 2, rows, DV), BF),
                pltpu.VMEM((2, nz // 2, 2, 4 * nz, DV), F32),
                pltpu.VMEM((2, nz, DV), F32),
                pltpu.VMEM((rows, width), F32),
                pltpu.VMEM((2, nz, 2, rows, 1), F32),
                pltpu.VMEM((2, nz, 2, rows, 1), F32),
                pltpu.VMEM((2, nz, 2, rows, DV), F32),
                pltpu.VMEM((heads, rows, rows), BF),
                pltpu.VMEM((heads, rows, DV), F32),
                pltpu.VMEM((heads, rows, DV), BF),
                pltpu.VMEM((heads, DV, DV), BF),
                pltpu.VMEM((ny, heads, slr, DV), BF),
                pltpu.VMEM((heads, DV), F32),
                pltpu.VMEM((ny, heads, DV), F32),
                pltpu.VMEM((ny, heads, slr, DV), F32),
                pltpu.VMEM((heads, slr, DV), BF),
                pltpu.VMEM((heads, DV), F32),
                pltpu.VMEM((nz, heads, slr, DV), BF),
                pltpu.VMEM((nz, heads, DV), F32),
                pltpu.VMEM((ny, heads, slr, DV), BF),
                pltpu.VMEM((heads, DV, DV), BF),
                dma, dma((6,)), dma, dma((2,)),
                dma((2, 2)), dma((2,)), dma((2, 2)), dma, dma, dma((3,)), dma((3,)),
                dma, dma, dma, dma, dma, dma, dma((2, 2, 2)),
                dma, dma((2, 2, hmax, 2)), dma, dma,
                dma((nz,)), dma((2, nz // 2)), dma((2,)), dma((2,)), dma, dma,
                dma, dma, dma, dma, dma, dma, dma, dma, dma, dma,
                dma, dma,
            ],
            compiler_params=pltpu.CompilerParams(
                collective_id=0, has_side_effects=True, vmem_limit_bytes=56 * 1024 * 1024
            ),
            name="mixer",
        )(
            tokens, in_gain[None], wq.T, wk.T, wvv.T, wrq.T, wrf.T, wri.T, lam[None], lower, scale[None],
            att_gain[None], rec_gain[None], aow, row_w,
        )
        return pl.pallas_call(
            finish,
            out_shape=(
                jax.ShapeDtypeStruct((rows, width), BF),
                jax.ShapeDtypeStruct((heads, rows), F32),
            ),
            in_specs=[vm, vm],
            out_specs=(vm, vm),
            compiler_params=pltpu.CompilerParams(vmem_limit_bytes=8 * 1024 * 1024),
            name="finish",
        )(parts, lse)

    col = P(None, ("tp", "fs"))
    return jax.shard_map(
        on_device,
        mesh=mesh,
        in_specs=(
            P(("fs", "sp"), None), P(), col, col, col, col, col, col,
            P("tp"), P("tp", None), P(("fs", "sp")), P(), P(), P("tp", None), P("tp", None),
        ),
        out_specs=(P(("fs", "sp"), None), P("tp", ("fs", "sp"))),
        check_vma=False,
    )
```

```python
import functools

import jax
import jax.numpy as jnp
from jax import lax
from jax.experimental import pallas as pl
from jax.experimental.pallas import tpu as pltpu
from jax.sharding import PartitionSpec as P

DK = 64
DV = 128
SUB = 16
EPS = 1e-06
NEG = -1e30
MESH = pl.DeviceIdType.MESH
BF = jnp.bfloat16
F32 = jnp.float32


def dot_nt(a, b):
    return lax.dot_general(a, b, (((1,), (1,)), ((), ())), preferred_element_type=jnp.float32)


def dot_nn(a, b):
    return jnp.dot(a, b, preferred_element_type=jnp.float32)


def grid_of(n_sp):
    ny = 1
    while ny * ny < n_sp:
        ny *= 2
    return n_sp // ny, ny


def kernel(
    n_sp, n_fs, n_tp,
    tok, gain_h, w0, w1, w2, w3, w4, w5, lam_h, lower_h, scale_h, att_gain_h, rec_gain_h, aow, row_w,
    parts, lse,
    tokv, gain, lam, lower, scale, att_gain, rec_gain, aov, rov, wcat, nown, near_a, near_c, far, psend, pr, kvp, q2, kvg, qb,
    osnd, orcv, stx, lsrow, prt, m_s, l_s, acc,
    smat, olocal, qdec, lsend, lrec, tl, trec, pre, tsnd, rdsnd, zrec, zrd, r3s, s_in,
    t_sem, g_sem, w_sem, wx_s, wx_r, o_sem, xa_r, xc_r, xf_r, x_s, xf_s, rel_s, rel_r,
    b_s, b_r, c_s, c_r, kp_s, k0_s, kp_r, kv_s, kv_r, q_s, q_r,
    os_s, os_r, sx_s, sx_r, sy_s, sy_r, r1_s, r1_r, r1t_s, r1t_r, r2_s, r2_r, r2t_s, r2t_r, r3_s, r3_r, op_s, op_r,
):
    nz, ny = grid_of(n_sp)
    hz = nz // 2
    sl_rows = DV // ny
    z, f, t = lax.axis_index("sp"), lax.axis_index("fs"), lax.axis_index("tp")
    i, j = z // ny, lax.rem(z, ny)
    mir = nz - 1 - i
    low = jnp.minimum(i, mir)
    hd = jnp.where(i < hz, 0, 1)
    rows, width = tok.shape
    half = rows // n_tp
    qr = half // 2
    hq = qr // 2
    heads = n_fs // 2
    right, left = lax.rem(f + 1, n_fs), lax.rem(f + n_fs - 1, n_fs)
    across = lax.rem(f + 2, n_fs)
    j_r, j_l = lax.rem(j + 1, ny), lax.rem(j + ny - 1, ny)

    def remote(src, dst, s, r, **dev):
        return pltpu.make_async_remote_copy(src, dst, s, r, device_id=dev, device_id_type=MESH)

    def landed(ref, sem):
        pltpu.make_async_copy(ref, ref, sem).wait()

    def sp_of(a, b):
        return a * ny + b

    tcopy = pltpu.make_async_copy(tok, tokv, t_sem)
    tcopy.start()
    scopies = [
        pltpu.make_async_copy(a, b, g_sem.at[n])
        for n, (a, b) in enumerate((
            (gain_h, gain), (lam_h, lam), (lower_h, lower), (scale_h, scale),
            (att_gain_h, att_gain), (rec_gain_h, rec_gain),
        ))
    ]
    for c in scopies:
        c.start()
    barrier = pltpu.get_barrier_semaphore()
    oth = n_tp - 1 - t
    for row in (i, mir):
        pl.semaphore_signal(
            barrier, inc=1, device_id={"fs": across, "sp": sp_of(row, j), "tp": oth}, device_id_type=MESH
        )
    for d in range(1, n_fs):
        peer = lax.rem(f + d, n_fs)
        pl.semaphore_signal(barrier, inc=1, device_id={"fs": peer}, device_id_type=MESH)
        pl.semaphore_signal(
            barrier, inc=1, device_id={"fs": peer, "sp": sp_of(mir, j)}, device_id_type=MESH
        )
    for d in range(1, n_tp):
        pl.semaphore_signal(barrier, inc=1, device_id={"tp": lax.rem(t + d, n_tp)}, device_id_type=MESH)
    for d in range(1, ny):
        pl.semaphore_signal(barrier, inc=1, device_id={"sp": sp_of(i, lax.rem(j + d, ny))}, device_id_type=MESH)
    for d in range(1, nz):
        pl.semaphore_signal(barrier, inc=1, device_id={"sp": sp_of(lax.rem(i + d, nz), j)}, device_id_type=MESH)

    wcopies = [
        pltpu.make_async_copy(w, wcat.at[pl.ds(DV + n * DK, DK)], w_sem)
        for n, w in enumerate((w1, w2, w0, w3, w4, w5))
    ]
    for c in wcopies:
        c.start()
    ocopies = [
        pltpu.make_async_copy(aow, aov, o_sem.at[0]),
        pltpu.make_async_copy(row_w, rov, o_sem.at[1]),
    ]

    blk = 32
    tcopy.wait()
    scopies[0].wait()

    @pl.loop(0, rows // blk)
    def _(n):
        sl = pl.ds(pl.multiple_of(n * blk, blk), blk)
        x = tokv[sl, :].astype(F32)
        ms = jnp.mean(x * x, axis=-1, keepdims=True)
        nown[sl, :] = (x * lax.rsqrt(ms + EPS) * gain[...]).astype(BF)

    m_s[...] = jnp.full(m_s.shape, NEG, F32)
    l_s[...] = jnp.zeros(l_s.shape, F32)
    acc[...] = jnp.zeros(acc.shape, F32)
    for k in range(1, hz):
        @pl.when(k > i)
        def _():
            for h in range(2):
                orcv[h, k] = jnp.zeros((rows, DV), BF)
    pl.semaphore_wait(barrier, 2 + 2 * (n_fs - 1) + n_tp - 1 + ny - 1 + nz - 1)

    def own_rows(at, size):
        return nown.at[pl.ds(pl.multiple_of(t * half + at, hq), size)]

    def send_a(way, n):
        return remote(
            own_rows(way * qr + n * hq, hq), near_a.at[way, t, pl.ds(n * hq, hq)],
            x_s, xa_r.at[way, n], fs=left if way else right,
        )

    def send_c(way):
        return remote(
            own_rows((1 - way) * qr, qr), near_c.at[way, t], x_s, xc_r.at[way], fs=left if way else right
        )

    def send_f(way, n):
        at = pl.ds(n * hq, hq)
        return remote(
            near_a.at[way, t, at], far.at[t, way, at], xf_s, xf_r.at[way, n], fs=left if way else right
        )

    for n in range(2):
        for way in range(2):
            send_a(way, n).start()
    for way in range(2):
        send_c(way).start()
    for c in ocopies:
        c.start()

    def relay(idx, at):
        for e in range(1, n_tp):
            remote(at, at, rel_s.at[idx], rel_r.at[idx], tp=lax.rem(t + e, n_tp)).start()

    def relayed(idx, at):
        if n_tp > 1:
            landed(at, rel_r.at[idx])

    def project(x):
        return dot_nt(x.reshape(rows, width), wcat[DV:]).astype(BF)

    def split(x):
        return x.reshape(n_tp, 2, qr, DV)

    landed(wcat.at[pl.ds(DV, 6 * DK)], w_sem)
    wx = remote(wcat.at[pl.ds(DV, DV)], wcat.at[pl.ds(0, DV)], wx_s, wx_r, tp=oth)
    wx.start()


    back = (f, left, right, across)
    part = lax.rem(f, 2)
    mine = f // 2 == hd
    row_to = jnp.where(mine, i, mir)

    def kv_copy(slot, a):
        return remote(
            psend.at[slot, 0, :, a], kvp.at[hd, part, :, a], kp_s if slot else k0_s, kp_r.at[hd, part, a],
            sp=sp_of(row_to, j), fs=back[slot],
        )

    def q_part(slot, a):
        return remote(psend.at[slot, 1, :, a], pr.at[f, 0, :, a], b_s, b_r, fs=back[slot])

    def r_part(slot, a):
        return remote(psend.at[slot, 2, :, a], pr.at[f, 1, :, a], c_s, c_r, fs=back[slot])

    own = project(nown[...])
    pr[f, 0] = split(own[:, DV: 2 * DV])
    pr[f, 1] = split(own[:, 2 * DV:])

    @pl.when(mine)
    def _():
        kvp[hd, part] = split(own[:, :DV])

    @pl.when(jnp.logical_not(mine))
    def _():
        psend[0, 0] = split(own[:, :DV])
        for a in range(2):
            kv_copy(0, a).start()

    def deliver(todo, rest=()):
        for slot, a in todo:
            kv_copy(slot, a).start()
        for slot, a in rest:
            q_part(slot, a).start()
        for slot, a in rest:
            r_part(slot, a).start()

    def deliver_near(x, flip, rest):
        got = project(x)
        todo = []
        for way in range(2):
            a = 1 - way if flip else way
            for c in range(n_tp):
                lo = (way * n_tp + c) * qr
                for g in range(3):
                    psend[1 + way, g, c, a] = got[lo: lo + qr, g * DV: (g + 1) * DV]
            todo.append((1 + way, a))
        deliver(todo, rest)

    for n in range(2):
        for way in range(2):
            landed(near_a.at[way, t, pl.ds(n * hq, hq)], xa_r.at[way, n])
            send_f(way, n).start()
            relay(0, near_a.at[way, t, pl.ds(n * hq, hq)])
    relayed(0, near_a.at[:, oth])
    deliver_near(near_a[...], False, [])
    for way in range(2):
        landed(near_c.at[way, t], xc_r.at[way])
        relay(2, near_c.at[way, t])
    relayed(2, near_c.at[:, oth])
    deliver_near(near_c[...], True, [(1, 0), (2, 1)])
    for n in range(2):
        for way in range(2):
            landed(far.at[t, way, pl.ds(n * hq, hq)], xf_r.at[way, n])
            relay(1, far.at[t, way, pl.ds(n * hq, hq)])
    wx.wait_recv()
    got = dot_nt(far[t].reshape(half, width), wcat[: 2 * DV]).astype(BF)
    psend[3, 0, 0] = got[:, DV:].reshape(2, qr, DV)
    psend[3, 0, 1] = got[:, :DV].reshape(2, qr, DV)
    for n, core in enumerate((t, oth)):
        remote(
            psend.at[3, 0, n], kvp.at[hd, part, t], kp_s, kp_r.at[hd, part, t],
            sp=sp_of(row_to, j), fs=across, tp=core,
        ).start()
    relayed(1, far.at[oth])
    far_rows = far[...].reshape(rows, width)
    got = dot_nt(far_rows, wcat[2 * DV:]).astype(BF)
    for g in range(2):
        psend[3, 1 + g] = split(got[:, g * DV: (g + 1) * DV])
    deliver([], [(3, 0), (3, 1), (1, 1), (2, 0)])

    def flat(x):
        return x.reshape(rows, DV)

    def pair(h, g, lo):
        return jnp.concatenate([flat(pr[2 * h + p, g])[:, lo: lo + DK] for p in range(2)], axis=1)

    slot_of = (hd, 1 - hd)

    def gather_kv(role):
        g = slot_of[role]
        for p in range(2):
            @pl.when((role == 1) | (2 * hd + p != f))
            def _():
                for a in range(2):
                    landed(kvp.at[g, p, :, a], kp_r.at[g, p, a])
        got = [flat(kvp[g, p]) for p in range(2)]
        kvg[g, j, :, :DV] = jnp.concatenate([x[:, :DK] for x in got], axis=1)
        kvg[g, j, :, DV:] = jnp.concatenate([x[:, DK:] for x in got], axis=1)

    right_hops = (ny // 2, ny - 1 - ny // 2)
    left_hops = (ny - 1 - ny // 2, ny // 2)

    half_k = rows // 2

    def block(role, way, d, n):
        return kvg.at[slot_of[role], lax.rem(j + (d if way else ny - d), ny), pl.ds(n * half_k, half_k)]

    def ring(role, way, d, n):
        at = block(role, way, d, n)
        return remote(at, at, kv_s, kv_r.at[role, way, d, n], sp=sp_of(i, j_l if way else j_r))

    hops = [(right_hops[g], left_hops[g]) for g in range(2)]

    taken = set()

    def step(g, d, again=False):
        if (g, d) in taken and not again:
            return
        taken.add((g, d))
        for n in range(2):
            for way in range(2):
                if 0 < d <= hops[g][way]:
                    landed(block(g, way, d, n), kv_r.at[g, way, d - 1, n])
                if d < hops[g][way]:
                    ring(g, way, d, n).start()

    gather_kv(0)
    step(0, 0)
    gather_kv(1)
    step(1, 0)

    landed(pr.at[pl.ds(0, n_fs - 1), 0], b_r)
    for h in range(heads):
        q2[h] = (pair(h, 0, 0).astype(F32) * DK ** (-0.5)).astype(BF)
    qb[i] = q2[hd]

    def q_copy(d):
        a = lax.rem(i + d, nz)
        return remote(q2.at[jnp.where(a < hz, 0, 1)], qb.at[i], q_s, q_r, sp=sp_of(a, j))

    def wanted(a):
        return (min(a, nz - 1 - a) <= i) & (i != a)

    for d in range(1, nz):
        q_copy(d).start()

    landed(pr.at[pl.ds(0, n_fs - 1), 1], c_r)

    ri_row = lax.broadcasted_iota(jnp.int32, (rows, DV), 0)
    lane = lax.broadcasted_iota(jnp.int32, (rows, DV), 1)
    sub_pos = lax.rem(ri_row, SUB)
    tri = (
        lax.broadcasted_iota(jnp.int32, (rows, rows), 0)
        >= lax.broadcasted_iota(jnp.int32, (rows, rows), 1)
    )
    trif = tri.astype(F32)
    gates = []
    for c in scopies[1:]:
        c.wait()
    sc = jnp.broadcast_to(scale[...], (DV, rows)).T
    for h in range(heads):
        rf = pair(h, 1, 0).astype(F32)
        ri = pair(h, 1, DK).astype(F32)
        lb = lower[h: h + 1, :]
        g = sc * jnp.log(lb + (1.0 - lb) * jax.nn.sigmoid(rf))
        kk = 1.0 - jnp.exp(g)
        a = jnp.dot(trif, g, preferred_element_type=F32, precision=lax.Precision.HIGHEST)
        last = a[rows - 1: rows, :]
        kd = (kk * jnp.exp(last - a)).astype(BF)
        lsend[h] = dot_nn(ri.T.astype(BF), kd).astype(BF)
        tl[h: h + 1, :] = jnp.exp(last)
        gates.append((a, kk, ri))

    def sl_of(y):
        return pl.ds(pl.multiple_of(y * sl_rows, sl_rows), sl_rows)

    def r1(d):
        y = lax.rem(j + d, ny)
        return (
            remote(lsend.at[:, sl_of(y)], lrec.at[j], r1_s, r1_r, sp=sp_of(i, y)),
            remote(tl, trec.at[j], r1t_s, r1t_r, sp=sp_of(i, y)),
        )

    lrec[j] = lsend[:, sl_of(j), :]
    trec[j] = tl[...]
    for d in range(1, ny):
        for c in r1(d):
            c.start()

    step(0, 1)
    step(1, 1)

    def local(h):
        a, kk, ri = gates[h]
        rq = pair(h, 0, DK).astype(F32)
        qdec[h] = (rq * jnp.exp(a)).astype(BF)
        smat[h, 0:SUB, :] = jnp.zeros((SUB, rows), BF)
        for n in range(1, rows // SUB):
            lo = n * SUB
            ref = a[lo - 1: lo, :]
            qd = (rq[lo: lo + SUB] * jnp.exp(a[lo: lo + SUB] - ref)).astype(BF)
            kd = (kk * jnp.exp(jnp.where(ri_row < lo, ref - a, NEG))).astype(BF)
            smat[h, lo: lo + SUB, :] = dot_nt(qd, kd).astype(BF)
        o = dot_nn(smat[h], ri.astype(BF))
        o = o + jnp.sum(rq * kk, axis=-1, keepdims=True) * ri
        for d in range(1, SUB):
            valid = sub_pos >= d
            dec = jnp.exp(jnp.where(valid, a - pltpu.roll(a, d, 0), NEG))
            col = jnp.sum(rq * dec * pltpu.roll(kk, d, 0), axis=-1, keepdims=True)
            o = o + col * pltpu.roll(ri, d, 0)
        olocal[h] = o

    local(0)
    local(1)
    diag = (
        lax.broadcasted_iota(jnp.int32, (rows, rows), 1)
        - lax.broadcasted_iota(jnp.int32, (rows, rows), 0)
    )

    def strip(chunk, blocks, groups, offs):
        kts, vts, masks = [], [], []
        for g, masked in groups:
            for o in offs:
                y = lax.rem(j + o, ny)
                kts.append(kvg[g, y, :, :DV])
                vts.append(kvg[g, y, :, DV:])
                masks.append(diag <= (j - y) * rows if masked else None)
        kt = jnp.concatenate(kts, axis=0)
        vt = jnp.concatenate(vts, axis=0)
        scores = []
        for b in blocks:
            q = qb[b]
            for m in range(2):
                scores.append(dot_nt(jnp.where((lane < DK) if m == 0 else (lane >= DK), q, jnp.zeros_like(q)), kt))
        done = []
        for sco in scores:
            if any(x is not None for x in masks):
                sco = jnp.concatenate([
                    sco[:, n * rows: (n + 1) * rows] if x is None
                    else jnp.where(x, sco[:, n * rows: (n + 1) * rows], NEG)
                    for n, x in enumerate(masks)
                ], axis=1)
            top = jnp.max(sco, axis=-1, keepdims=True)
            e = jnp.exp(sco - top)
            done.append((top, jnp.sum(e, axis=-1, keepdims=True), dot_nn(e.astype(BF), vt)))
        for n, (top, tot, num) in enumerate(done):
            b, m = blocks[n // 2], n % 2
            m_s[chunk, b, m] = top
            l_s[chunk, b, m] = tot
            acc[chunk, b, m] = num

    high = nz - 1 - low

    def sweep(chunk, dists, between=None):
        offs = sorted({o % ny for d in dists for o in (d, -d) if d <= ny // 2})
        if not offs:
            return

        strip(chunk, [low], [(0, True)], offs)

        @pl.loop(0, (high - low - 1) // 2)
        def _(n):
            strip(chunk, [low + 1 + 2 * n, low + 2 + 2 * n], [(0, False)], offs)

        if between is not None:
            pl.when(low < hz // 2)(between)
        strip(chunk, [high], [(0, False), (1, True)], offs)
        if between is not None:
            pl.when(low >= hz // 2)(between)

        @pl.loop(high + 1, nz)
        def _(b):
            strip(chunk, [b], [(0, False), (1, False)], offs)

    step(0, 2)
    step(1, 2)

    landed(lrec.at[pl.ds(0, ny - 1)], r1_r)
    landed(trec.at[pl.ds(0, ny - 1)], r1t_r)
    run = jnp.zeros((heads, sl_rows, DV), F32)
    rd = jnp.ones((heads, DV), F32)
    for y in range(ny):
        pre[y] = run
        run = trec[y][:, None, :] * run + lrec[y].astype(F32)
        rd = rd * trec[y]
    tsnd[...] = run.astype(BF)
    rdsnd[...] = rd

    def r2(d):
        to = sp_of(lax.rem(i + d, nz), j)
        return (
            remote(tsnd, zrec.at[i], r2_s, r2_r, sp=to),
            remote(rdsnd, zrd.at[i], r2t_s, r2t_r, sp=to),
        )

    for d in range(1, nz):
        for c in r2(d):
            c.start()

    landed(qb.at[pl.ds(0, nz - 1)], q_r)

    def row_of(h, k):
        return jnp.where(h == 0, k, nz - 1 - k)

    def stat_copy(chunk, d):
        at = stx.at[hd, low, chunk]
        return remote(at, at, sx_s.at[chunk], sx_r.at[chunk], sp=sp_of(row_of(hd, lax.rem(low + d, hz)), j))

    def emit(chunk):
        st = jnp.zeros((rows, DV), F32)
        for b in range(nz):
            for m in range(2):
                st = jnp.where(lane == m * nz + b, m_s[chunk, b, m], st)
                st = jnp.where(lane == (2 + m) * nz + b, l_s[chunk, b, m], st)
        stx[hd, low, chunk] = st.T[:4 * nz, :]
        for d in range(1, hz):
            stat_copy(chunk, d).start()

    def lse_copy(k):
        b = row_of(1 - hd, k)
        return remote(
            lsrow.at[hd, pl.ds(b, 1)], lsrow.at[hd, pl.ds(b, 1)], sy_s, sy_r, sp=sp_of(b, j)
        )

    def out_copy(b):
        return remote(osnd.at[b], orcv.at[hd, low], os_s.at[b], os_r.at[hd, low], sp=sp_of(b, j))

    def third():
        for g in range(2):
            step(g, 3, True)

    sweep(0, (0, 1, 2), between=third)
    emit(0)
    for d in range(3, ny // 2 + 1):
        for g in range(2):
            step(g, d)

    landed(zrec.at[pl.ds(0, nz - 1)], r2_r)
    landed(zrd.at[pl.ds(0, nz - 1)], r2t_r)
    run = jnp.zeros((heads, sl_rows, DV), F32)
    for a in range(nz - 1):
        run = jnp.where(a < i, zrd[a][:, None, :] * run + zrec[a].astype(F32), run)
    for y in range(ny):
        r3s[y] = (run + pre[y]).astype(BF)
        run = trec[y][:, None, :] * run

    def r3(d):
        y = lax.rem(j + d, ny)
        return remote(r3s.at[y], s_in.at[:, sl_of(j)], r3_s, r3_r, sp=sp_of(i, y))

    s_in[:, sl_of(j), :] = r3s[j]
    for d in range(1, ny):
        r3(d).start()

    sweep(1, range(3, ny // 2 + 1))
    emit(1)

    lam_h = jnp.where(hd == 0, lam[0, 0], lam[0, 1])

    def send_out(b, num):
        @pl.when(b == i)
        def _():
            orcv[hd, low] = num

        @pl.when(b != i)
        def _():
            osnd[b] = num
            out_copy(b).start()

    @pl.when(low == 0)
    def _():
        weights = []
        for m in range(2):
            tops = [stx[hd, 0, chunk, m * nz: m * nz + 1, :] for chunk in range(2)]
            tots = [stx[hd, 0, chunk, (2 + m) * nz: (2 + m) * nz + 1, :] for chunk in range(2)]
            top = jnp.maximum(tops[0], tops[1])
            scales = [jnp.exp(x - top) for x in tops]
            total = scales[0] * tots[0] + scales[1] * tots[1]
            for x in scales:
                weights.append(-lam_h * (x / total) if m else x / total)
        wt = jnp.concatenate(weights + [jnp.zeros((DV - 4, DV), F32)], axis=0).T
        num = jnp.zeros((rows, DV), F32)
        for m in range(2):
            for chunk in range(2):
                at = 2 * m + chunk
                num = num + acc[chunk, 0, m] * wt[:, at: at + 1]
        send_out(0, num.astype(BF))

    landed(r3s.at[pl.ds(0, ny - 1)], r3_r)
    recs = []
    rg = rec_gain[...]
    for h in range(heads):
        o = olocal[h] + dot_nt(qdec[h], s_in[h])
        ms = jnp.mean(o * o, axis=-1, keepdims=True)
        recs.append((o * lax.rsqrt(ms + EPS) * rg).astype(BF))
    rec = jnp.concatenate(recs, axis=1)
    for c in ocopies:
        c.wait()
    pieces = 4
    cols = width // pieces
    for n in range(pieces):
        sl = slice(n * cols, (n + 1) * cols)
        prt[:, sl] = dot_nn(rec, rov[:, sl])

    if hz > 1:
        for chunk in range(2):
            landed(stx.at[0, pl.ds(0, hz - 1), chunk], sx_r.at[chunk])

    def stat(k, chunk, r):
        return stx[hd, k, chunk, r * nz: (r + 1) * nz, :]

    sources = [(k, chunk) for k in range(hz) for chunk in range(2)]
    weights = []
    for m in range(2):
        top = stat(0, 0, m)
        for k, chunk in sources[1:]:
            top = jnp.maximum(top, stat(k, chunk, m))
        total = jnp.zeros((nz, DV), F32)
        for k, chunk in sources:
            total = total + jnp.exp(stat(k, chunk, m) - top) * stat(k, chunk, 2 + m)
        if m == 0:
            lsrow[hd] = top + jnp.log(total)
        for chunk in range(2):
            wt = jnp.exp(stx[hd, low, chunk, pl.ds(m * nz, nz), :] - top) / total
            weights.append(-lam_h * wt if m else wt)

    @pl.when(low == 0)
    def _():
        for k in range(hz):
            lse_copy(k).start()

    wt = jnp.concatenate(weights + [jnp.zeros((DV - 4 * nz, DV), F32)], axis=0).T
    for b in range(1, nz):
        @pl.when(b >= low)
        def _():
            num = jnp.zeros((rows, DV), F32)
            for m in range(2):
                for chunk in range(2):
                    at = (2 * m + chunk) * nz + b
                    num = num + acc[chunk, b, m] * wt[:, at: at + 1]
            send_out(b, num.astype(BF))

    landed(lsrow.at[0, pl.ds(0, 1)], sy_r)
    for k in range(hz):
        for h in range(2):
            @pl.when((k <= i) & ((hd != h) | (low != k)))
            def _():
                landed(orcv.at[h, k], os_r.at[h, k])

    atts = []
    ag = att_gain[...]
    for h in range(heads):
        lse[h: h + 1, :] = lsrow[h, pl.ds(i, 1), :]
        x = orcv[h, 0].astype(F32)
        for k in range(1, hz):
            x = x + orcv[h, k].astype(F32)
        ms = jnp.mean(x * x, axis=-1, keepdims=True)
        atts.append((x * lax.rsqrt(ms + EPS) * ag * 0.8).astype(BF))
    att = jnp.concatenate(atts, axis=1)

    for n in range(pieces):
        sl = slice(n * cols, (n + 1) * cols)
        parts[0, :, sl] = (dot_nn(att, aov[:, sl]) + prt[:, sl]).astype(BF)
        for e in range(1, n_tp):
            c = remote(
                parts.at[0, :, sl], parts.at[e, :, sl], op_s, op_r,
                tp=lax.rem(t + e, n_tp),
            )
            c.start()

    landed(nown, x_s)
    wx.wait_send()
    landed(near_a.at[:, 0], xf_s)
    if n_tp > 1:
        landed(near_a.at[:, 0], rel_s.at[0])
        landed(far.at[0], rel_s.at[1])
        landed(near_c.at[:, 0], rel_s.at[2])
    landed(psend.at[pl.ds(1, n_fs - 1), 0], kp_s)
    landed(psend.at[pl.ds(1, n_fs - 1), 1], b_s)
    landed(psend.at[pl.ds(1, n_fs - 1), 2], c_s)

    @pl.when(jnp.logical_not(mine))
    def _():
        landed(psend.at[0, 0], k0_s)

    landed(kvg.at[:, pl.ds(0, ny - 1)], kv_s)
    landed(qb.at[pl.ds(0, nz - 1)], q_s)
    landed(lrec.at[pl.ds(0, ny - 1)], r1_s)
    landed(trec.at[pl.ds(0, ny - 1)], r1t_s)
    landed(zrec.at[pl.ds(0, nz - 1)], r2_s)
    landed(zrd.at[pl.ds(0, nz - 1)], r2t_s)
    landed(r3s.at[pl.ds(0, ny - 1)], r3_s)
    if hz > 1:
        for chunk in range(2):
            landed(stx.at[0, pl.ds(0, hz - 1), chunk], sx_s.at[chunk])

    @pl.when(low == 0)
    def _():
        landed(lsrow.at[0, pl.ds(0, hz)], sy_s)

    for a in range(nz):
        @pl.when((a >= low) & (i != a))
        def _():
            out_copy(a).wait_send()
    if n_tp > 1:
        landed(parts.at[0], op_s)
        landed(parts.at[1], op_r)


def finish(parts, lse_in, mixed, lse):
    total = parts[0].astype(jnp.float32)
    for e in range(1, parts.shape[0]):
        total = total + parts[e].astype(jnp.float32)
    mixed[...] = total.astype(jnp.bfloat16)
    lse[...] = lse_in[...]


def solution(mesh):
    n_sp, n_fs, n_tp = (mesh.shape[k] for k in ("sp", "fs", "tp"))
    nz, ny = grid_of(n_sp)

    def on_device(
        tokens, in_gain, wq, wk, wvv, wrq, wrf, wri, lam, lower, scale, att_gain, rec_gain, aow, row_w
    ):
        rows, width = tokens.shape
        heads = lower.shape[0]
        assert heads == 2 and n_fs == 4 and n_tp == 2 and rows == DV and nz % 2 == 0
        vm = pl.BlockSpec(memory_space=pltpu.VMEM)
        hbm = pl.BlockSpec(memory_space=pltpu.HBM)
        dma = pltpu.SemaphoreType.DMA
        qr = rows // (2 * n_tp)
        slr = DV // ny
        hmax = max(ny // 2, 1)
        parts, lse = pl.pallas_call(
            functools.partial(kernel, n_sp, n_fs, n_tp),
            out_shape=(pltpu.VMEM((n_tp, rows, width), BF), pltpu.VMEM((heads, rows), F32)),
            in_specs=[hbm] * 15,
            out_specs=(vm, vm),
            scratch_shapes=[
                pltpu.VMEM(tokens.shape, BF),
                pltpu.VMEM((1, width), F32),
                pltpu.SMEM((1, heads), F32),
                pltpu.VMEM((heads, DV), F32),
                pltpu.VMEM((1, rows), F32),
                pltpu.VMEM((1, DV), F32),
                pltpu.VMEM((1, DV), F32),
                pltpu.VMEM(aow.shape, BF),
                pltpu.VMEM(row_w.shape, BF),
                pltpu.VMEM((DV + 6 * DK, width), BF),
                pltpu.VMEM((rows, width), BF),
                pltpu.VMEM((2, n_tp, qr, width), BF),
                pltpu.VMEM((2, n_tp, qr, width), BF),
                pltpu.VMEM((n_tp, 2, qr, width), BF),
                pltpu.VMEM((n_fs, 3, n_tp, 2, qr, DV), BF),
                pltpu.VMEM((n_fs, 2, n_tp, 2, qr, DV), BF),
                pltpu.VMEM((2, 2, n_tp, 2, qr, DV), BF),
                pltpu.VMEM((heads, rows, DV), BF),
                pltpu.VMEM((2, ny, rows, 2 * DV), BF),
                pltpu.VMEM((nz, rows, DV), BF),
                pltpu.VMEM((nz, rows, DV), BF),
                pltpu.VMEM((2, nz // 2, rows, DV), BF),
                pltpu.VMEM((2, nz // 2, 2, 4 * nz, DV), F32),
                pltpu.VMEM((2, nz, DV), F32),
                pltpu.VMEM((rows, width), F32),
                pltpu.VMEM((2, nz, 2, rows, 1), F32),
                pltpu.VMEM((2, nz, 2, rows, 1), F32),
                pltpu.VMEM((2, nz, 2, rows, DV), F32),
                pltpu.VMEM((heads, rows, rows), BF),
                pltpu.VMEM((heads, rows, DV), F32),
                pltpu.VMEM((heads, rows, DV), BF),
                pltpu.VMEM((heads, DV, DV), BF),
                pltpu.VMEM((ny, heads, slr, DV), BF),
                pltpu.VMEM((heads, DV), F32),
                pltpu.VMEM((ny, heads, DV), F32),
                pltpu.VMEM((ny, heads, slr, DV), F32),
                pltpu.VMEM((heads, slr, DV), BF),
                pltpu.VMEM((heads, DV), F32),
                pltpu.VMEM((nz, heads, slr, DV), BF),
                pltpu.VMEM((nz, heads, DV), F32),
                pltpu.VMEM((ny, heads, slr, DV), BF),
                pltpu.VMEM((heads, DV, DV), BF),
                dma, dma((6,)), dma, dma, dma, dma((2,)),
                dma((2, 2)), dma((2,)), dma((2, 2)), dma, dma, dma((3,)), dma((3,)),
                dma, dma, dma, dma, dma, dma, dma((2, 2, 2)),
                dma, dma((2, 2, hmax, 2)), dma, dma,
                dma((nz,)), dma((2, nz // 2)), dma((2,)), dma((2,)), dma, dma,
                dma, dma, dma, dma, dma, dma, dma, dma, dma, dma,
                dma, dma,
            ],
            compiler_params=pltpu.CompilerParams(
                collective_id=0, has_side_effects=True, vmem_limit_bytes=56 * 1024 * 1024
            ),
            name="mixer",
        )(
            tokens, in_gain[None], wq.T, wk.T, wvv.T, wrq.T, wrf.T, wri.T, lam[None], lower, scale[None],
            att_gain[None], rec_gain[None], aow, row_w,
        )
        return pl.pallas_call(
            finish,
            out_shape=(
                jax.ShapeDtypeStruct((rows, width), BF),
                jax.ShapeDtypeStruct((heads, rows), F32),
            ),
            in_specs=[vm, vm],
            out_specs=(vm, vm),
            compiler_params=pltpu.CompilerParams(vmem_limit_bytes=8 * 1024 * 1024),
            name="finish",
        )(parts, lse)

    col = P(None, ("tp", "fs"))
    return jax.shard_map(
        on_device,
        mesh=mesh,
        in_specs=(
            P(("fs", "sp"), None), P(), col, col, col, col, col, col,
            P("tp"), P("tp", None), P(("fs", "sp")), P(), P(), P("tp", None), P("tp", None),
        ),
        out_specs=(P(("fs", "sp"), None), P("tp", ("fs", "sp"))),
        check_vma=False,
    )
```
